512 devices in a mesh: rep: 2 (over z_hi), fs: 32 (over z_lo, y), tp: 8 (over x, core).
Axes of the slice: x: 4, y: 8, z: 8 (z_hi: 2, z_lo: 4; z = z_hi * 4 + z_lo), core: 2. Of those that a mesh axis runs over, the one named last changes fastest.
Arguments:
- pre_gate: bfloat16 [49152, 4096], P(('rep', 'fs'), 'tp'), may hold values from -6 to 6
- pre_linear: bfloat16 [49152, 4096], P(('rep', 'fs'), 'tp'), may hold values from -6 to 6
- taps_gate: float32 [3, 4096], P(None, 'tp'), may hold values from -3.5 to 3.5
- taps_linear: float32 [3, 4096], P(None, 'tp'), may hold values from -3.5 to 3.5
- bias_gate: float32 [4096], P('tp'), may hold values from -3 to 3
- bias_linear: float32 [4096], P('tp'), may hold values from -3 to 3
- down_weight: bfloat16 [4096, 2048], P('tp', 'fs'), may hold values from -0.09375 to 0.09375
- out_grad: bfloat16 [49152, 2048], P(('rep', 'fs')), may hold values from -8 to 8
Outputs:
- grad_gate: bfloat16 [49152, 4096], P(('rep', 'fs'), 'tp')
- grad_linear: bfloat16 [49152, 4096], P(('rep', 'fs'), 'tp')
- grad_taps_gate: float32 [3, 4096], P(None, 'tp')
- grad_taps_linear: float32 [3, 4096], P(None, 'tp')
- grad_bias_gate: float32 [4096], P('tp')
- grad_bias_linear: float32 [4096], P('tp')
- grad_down: float32 [4096, 2048], P('tp', 'fs')
- row_norms: float32 [4096], P('tp')
The draws below stay inside these ranges and needn't reach their ends.
All inputs are finite; a program needn't handle non-finite values.
Results may differ from the reference program's by a relative error of at most 0.0031.
Values may be sent and summed in bfloat16 or wider, within the bound.
A program may use at most 64 MiB of HBM per device.

```python
import jax
import jax.numpy as jnp

D = 2048
FF = 4096
KERNEL = 3
TOK_DEV = 768
TOKENS = 49152


def raised(entries, key, source, target, blocks, factor):
    owner, partner = [(jnp.arange(entries.shape[axis_at]) // (entries.shape[axis_at] // blocks)).reshape([-1 if axis == axis_at else 1 for axis in range(entries.ndim)]) for axis_at in (source, target)]
    chosen = jax.random.permutation(key, blocks)[partner]
    strong = (owner == chosen) | (owner == (partner + blocks // 2) % blocks)
    return jnp.where(strong, factor * entries, entries)


def levels(rng, dims, cuts, low, high):
    gain, own = 1.0, jax.random.fold_in(rng, 6)
    for position, blocks in cuts:
        draws = jnp.exp(jax.random.uniform(jax.random.fold_in(own, position), (blocks,), jnp.float32, low / len(cuts), high / len(cuts)))
        gain = gain * jnp.repeat(draws, dims[position] // blocks).reshape([-1 if axis == position else 1 for axis in range(len(dims))])
    return gain


def bell_draw(own_key, shape, scale, limit, shards=(), kind=jnp.bfloat16):
    entries = scale * jax.random.normal(own_key, shape, jnp.float32)
    if shards:
        entries = entries * levels(own_key, shape, shards, -0.22, 0.18)
    return jnp.clip(entries, -limit, limit).astype(kind)


def heavy_noise(key, dims, deviation, most, pieces, heavy, kind=jnp.bfloat16):
    entries = deviation * jax.random.normal(key, dims, jnp.float32)
    if pieces:
        entries = entries * levels(key, dims, pieces, -0.22, 0.18)
    return jnp.clip(raised(entries, jax.random.fold_in(key, 3), *heavy), -most, most).astype(kind)


def setup_inputs(seed: int = 0) -> dict:
    seeds = jax.random.split(jax.random.key(seed), 9)
    return {
        "pre_gate": bell_draw(seeds[0], (TOKENS, FF), 1.0, 6.0, ((0, 64), (1, 8))),
        "pre_linear": bell_draw(seeds[1], (TOKENS, FF), 1.0, 6.0, ((0, 64), (1, 8))),
        "taps_gate": bell_draw(seeds[2], (KERNEL, FF), KERNEL ** -0.5, 3.5, ((1, 8),), jnp.float32),
        "taps_linear": bell_draw(seeds[3], (KERNEL, FF), KERNEL ** -0.5, 3.5, ((1, 8),), jnp.float32),
        "bias_gate": bell_draw(seeds[4], (FF,), 0.5, 3.0, ((0, 8),), jnp.float32),
        "bias_linear": bell_draw(seeds[5], (FF,), 0.5, 3.0, ((0, 8),), jnp.float32),
        "down_weight": bell_draw(seeds[6], (FF, D), FF ** -0.5, 0.09375, ((0, 8), (1, 32))),
        "out_grad": heavy_noise(seeds[7], (TOKENS, D), 1.0, 8.0, ((0, 64),), (0, 1, 64, 4.0)),
    }


def convolve(values, taps, bias):
    length = values.shape[1]
    padded = jnp.pad(values, ((0, 0), (2, 0), (0, 0)))
    return taps[0] * padded[:, 0:length] + taps[1] * padded[:, 1:length + 1] + taps[2] * padded[:, 2:length + 2] + bias


def convolve_back(grads, taps):
    length = grads.shape[1]
    padded = jnp.pad(grads, ((0, 0), (0, 2), (0, 0)))
    return taps[0] * padded[:, 2:length + 2] + taps[1] * padded[:, 1:length + 1] + taps[2] * padded[:, 0:length]


def tap_grads(grads, values):
    length = values.shape[1]
    padded = jnp.pad(values, ((0, 0), (2, 0), (0, 0)))
    return jnp.stack([jnp.sum(grads * padded[:, j:j + length], axis=(0, 1)) for j in range(3)])


def reference(pre_gate, pre_linear, taps_gate, taps_linear, bias_gate, bias_linear, down_weight, out_grad):
    seqs = pre_gate.shape[0] // TOK_DEV
    width = pre_gate.shape[1]
    gate_in = pre_gate.astype(jnp.float32).reshape(seqs, TOK_DEV, width)
    linear_in = pre_linear.astype(jnp.float32).reshape(seqs, TOK_DEV, width)
    gate_pre = convolve(gate_in, taps_gate, bias_gate)
    linear_pre = convolve(linear_in, taps_linear, bias_linear)
    sigma = jax.nn.sigmoid(gate_pre)
    silu_val = gate_pre * sigma
    hidden = (silu_val * linear_pre).astype(jnp.bfloat16).reshape(seqs * TOK_DEV, width)
    grad_hidden = jnp.dot(out_grad, down_weight.T, preferred_element_type=jnp.float32).reshape(seqs, TOK_DEV, width)
    grad_gate_pre = grad_hidden * linear_pre * sigma * (1.0 + gate_pre * (1.0 - sigma))
    grad_linear_pre = grad_hidden * silu_val
    grad_gate = convolve_back(grad_gate_pre, taps_gate).reshape(seqs * TOK_DEV, width).astype(jnp.bfloat16)
    grad_linear = convolve_back(grad_linear_pre, taps_linear).reshape(seqs * TOK_DEV, width).astype(jnp.bfloat16)
    grad_taps_gate = tap_grads(grad_gate_pre, gate_in)
    grad_taps_linear = tap_grads(grad_linear_pre, linear_in)
    grad_bias_gate = jnp.sum(grad_gate_pre, axis=(0, 1))
    grad_bias_linear = jnp.sum(grad_linear_pre, axis=(0, 1))
    grad_down = jnp.dot(hidden.T, out_grad, preferred_element_type=jnp.float32)
    row_norms = jnp.sum(grad_down * grad_down, axis=1)
    return (grad_gate, grad_linear, grad_taps_gate, grad_taps_linear, grad_bias_gate, grad_bias_linear, grad_down, row_norms)
```

```python
import jax
import jax.numpy as jnp
from jax import lax
from jax.experimental import pallas as pl
from jax.experimental.pallas import tpu as pltpu
from jax.sharding import Mesh
from jax.sharding import PartitionSpec as P

REP_FS = ("rep", "fs_0", "fs_1")
RING = 8
BLOCK = 64
HALF = 256
ROWS = 32
F32, BF16 = jnp.float32, jnp.bfloat16
FAR_FIRST = (4, 3, 5, 2, 6, 1, 7)


def gather_messages():
    found = []

    def add(half, dz, dy, part, axis, sign, needs):
        found.append((half, dz, dy, part, axis, sign, needs))
        return len(found) - 1

    right = add(0, 0, 0, 0, "z", 1, ())
    left = add(0, 0, 0, 0, "z", -1, ())
    right2 = add(0, -1, 0, 1, "z", 1, (right,))
    left2 = add(0, 1, 0, 2, "z", -1, (left,))
    for j, (dz, needs) in enumerate(
        ((0, ()), (-1, (right,)), (1, (left,)), (2, (right2, left2)))
    ):
        for sign, hops in ((1, 4 - j % 2), (-1, 3 + j % 2)):
            before = needs
            for k in range(hops):
                before = (add(0, dz, -sign * k, 0, "y", sign, before),)
    items = [(0, ())]
    for sign, hops in ((1, 4), (-1, 3)):
        before = ()
        for k in range(hops):
            before = (add(1, 0, -sign * k, 0, "y", sign, before),)
            items.append((-sign * (k + 1), before))
    for i, (dy, needs) in enumerate(items):
        first = add(1, 0, dy, 0, "z", 1, needs)
        other = add(1, 0, dy, 0, "z", -1, needs)
        if i % 2 == 0:
            add(1, -1, dy, 0, "z", 1, (first,))
        else:
            add(1, 1, dy, 0, "z", -1, (other,))
    return found


GATHER = gather_messages()
ROUND = []
for _m in GATHER:
    ROUND.append(1 + max((ROUND[k] for k in _m[6]), default=-1))
LAST_ROUND = max(ROUND)


def chain_messages():
    return [
        (half, part, sign, step, hops)
        for half in range(2)
        for part in range(2)
        for sign, hops in ((1, 4 - part), (-1, 3 + part))
        for step in range(hops)
    ]


CHAIN = chain_messages()
CHAIN_AT = {m[:4]: k for k, m in enumerate(CHAIN)}


def kernel(
    gate_hbm, linear_hbm, taps_g, taps_l, bias_g, bias_l, weight_hbm, out_grad_hbm,
    gg_hbm, gl_hbm, taps_g_out, taps_l_out, bias_g_out, bias_l_out, down_out, norms_out,
    gate, linear, out_grad, weights, hidden, factor_g, factor_l, grad_hidden, partial,
    gg, gl, chain_send, chain_recv, summed, cross_send, cross_recv, final, other_final,
    conv_send, conv_y, conv_z, norm_send, norm_y, norm_z,
    load_sem, store_sem, gather_s, gather_r, chain_s, chain_r, cross_s, cross_r,
    small_s, small_r, swap_s, swap_r,
):
    tokens = gate_hbm.shape[0]
    rep, z_lo, y = lax.axis_index("rep"), lax.axis_index("fs_0"), lax.axis_index("fs_1")
    z = rep * 4 + z_lo

    def along(axis, shift):
        if axis == "y":
            return {"fs_1": lax.rem(y + shift + RING, RING)}
        at = lax.rem(z + shift + RING, RING)
        return {"rep": at // 4, "fs_0": lax.rem(at, 4)}

    def remote(src, dst, send, recv, axis, shift):
        return pltpu.make_async_remote_copy(
            src_ref=src, dst_ref=dst, send_sem=send, recv_sem=recv,
            device_id=along(axis, shift), device_id_type=pl.DeviceIdType.MESH,
        )

    barrier = pltpu.get_barrier_semaphore()
    for axis in ("y", "z"):
        for shift in range(1, RING):
            pl.semaphore_signal(
                barrier, inc=1, device_id=along(axis, shift),
                device_id_type=pl.DeviceIdType.MESH,
            )

    own_row = pl.multiple_of((z_lo * 8 + y) * BLOCK, BLOCK)
    loads = [
        pltpu.make_async_copy(
            weight_hbm.at[:, pl.ds(h * HALF, HALF)],
            weights.at[h, pl.ds(own_row, BLOCK), :],
            load_sem.at[h],
        )
        for h in range(2)
    ]
    loads += [
        pltpu.make_async_copy(gate_hbm, gate.at[pl.ds(16, tokens), :], load_sem.at[2]),
        pltpu.make_async_copy(linear_hbm, linear.at[pl.ds(16, tokens), :], load_sem.at[3]),
        pltpu.make_async_copy(out_grad_hbm, out_grad, load_sem.at[4]),
    ]
    for load in loads:
        load.start()
    for ref in (gate, linear):
        ref[0:16, :] = jnp.zeros((16, ref.shape[1]), BF16)

    def gather_copy(k):
        half, dz, dy, part, axis, sign, _ = GATHER[k]
        at = lax.rem(z_lo + dz + 4, 4) * 8 + lax.rem(y + dy + RING, RING)
        start, size = at * BLOCK, BLOCK
        if part:
            start, size = start + (part - 1) * 32, 32
        block = weights.at[half, pl.ds(pl.multiple_of(start, size), size), :]
        return remote(block, block, gather_s.at[k], gather_r.at[k], axis, sign)

    def gather_round(number):
        arrived = set(k for k, r in enumerate(ROUND) if r < number - 1)
        todo = [k for k, r in enumerate(ROUND) if r == number]
        for k in [k for k, r in enumerate(ROUND) if r == number - 1]:
            gather_copy(k).wait_recv()
            arrived.add(k)
            for m in list(todo):
                if all(n in arrived for n in GATHER[m][6]):
                    gather_copy(m).start()
                    todo.remove(m)
        for m in todo:
            gather_copy(m).start()

    STEP = 32

    def shifted(ref, row, lanes):
        rows = ref[pl.ds(row, STEP + 16), lanes].astype(F32)
        return pltpu.roll(rows, 2, 0)[16:], pltpu.roll(rows, 1, 0)[16:], rows[16:]

    def forward(half):
        lanes = slice(half * HALF, (half + 1) * HALF)
        tg, tl = taps_g[0:3, lanes], taps_l[0:3, lanes]
        bg, bl = bias_g[0:1, lanes], bias_l[0:1, lanes]

        def body(i, carry):
            row = pl.multiple_of(i * STEP, STEP)
            g0, g1, g2 = shifted(gate, row, lanes)
            l0, l1, l2 = shifted(linear, row, lanes)
            gate_pre = tg[0:1] * g0 + tg[1:2] * g1 + tg[2:3] * g2 + bg
            linear_pre = tl[0:1] * l0 + tl[1:2] * l1 + tl[2:3] * l2 + bl
            sigma = 1.0 / (1.0 + jnp.exp(-gate_pre))
            silu = gate_pre * sigma
            hidden[pl.ds(row, STEP), lanes] = (silu * linear_pre).astype(BF16)
            factor_g[pl.ds(row, STEP), lanes] = (
                linear_pre * sigma * (1.0 + gate_pre * (1.0 - sigma))
            )
            factor_l[pl.ds(row, STEP), lanes] = silu
            return carry

        lax.fori_loop(0, tokens // STEP, body, 0)

    def weight_grad(half):
        lanes = slice(half * HALF, (half + 1) * HALF)

        def body(i, carry):
            at = pl.multiple_of(i * 512, 512)
            partial[half, pl.ds(at, 512), :] = lax.dot_general(
                out_grad[:, pl.ds(at, 512)], hidden[:, lanes],
                (((0,), (0,)), ((), ())), preferred_element_type=F32,
            )
            return carry

        lax.fori_loop(0, 4, body, 0)

    def hidden_grad(half):
        lanes = slice(half * HALF, (half + 1) * HALF)

        def body(i, carry):
            at = pl.multiple_of(i * 256, 256)
            grad_hidden[pl.ds(at, 256), lanes] = jnp.dot(
                out_grad[pl.ds(at, 256), :], weights[half], preferred_element_type=F32
            )
            return carry

        lax.fori_loop(0, tokens // 256, body, 0)

    def fold(v):
        return jnp.sum(v.reshape(STEP // 8, 8, HALF), axis=0)

    def backward(half):
        lanes = slice(half * HALF, (half + 1) * HALF)
        tg, tl = taps_g[0:3, lanes], taps_l[0:3, lanes]

        def back(v, after, taps):
            longer = jnp.concatenate([v, after], axis=0)
            one = pltpu.roll(longer, STEP + 7, 0)[0:STEP]
            two = pltpu.roll(longer, STEP + 6, 0)[0:STEP]
            return taps[0:1] * two + taps[1:2] * one + taps[2:3] * v

        def body(i, carry):
            after_g, after_l, sums = carry
            row = pl.multiple_of((tokens // STEP - 1 - i) * STEP, STEP)
            grad = grad_hidden[pl.ds(row, STEP), lanes]
            dg = grad * factor_g[pl.ds(row, STEP), lanes]
            dl = grad * factor_l[pl.ds(row, STEP), lanes]
            gs = shifted(gate, row, lanes)
            ls = shifted(linear, row, lanes)
            gg[pl.ds(row, STEP), lanes] = back(dg, after_g, tg).astype(BF16)
            gl[pl.ds(row, STEP), lanes] = back(dl, after_l, tl).astype(BF16)
            terms = [dg * v for v in gs] + [dl * v for v in ls] + [dg, dl]
            sums = tuple(s + fold(t) for s, t in zip(sums, terms))
            return dg[0:8], dl[0:8], sums

        zero = jnp.zeros((8, HALF), F32)
        _, _, sums = lax.fori_loop(0, tokens // STEP, body, (zero, zero, (zero,) * 8))
        for j, s in enumerate(sums):
            conv_send[j : j + 1, lanes] = jnp.sum(s, axis=0, keepdims=True)

    def first_axis(half):
        return ("y", y) if half == 0 else ("z", z)

    def pieces(half, to, part):
        if half == 0:
            return [((2 * part + q) * 512 + to * 64, 64) for q in range(2)]
        return [
            (lax.rem(to, 4) * 512 + (4 * part + q) * 64 + (to // 4) * 32, 32)
            for q in range(4)
        ]

    def chain_copy(k):
        half, part, sign, step, hops = CHAIN[k]
        return remote(
            chain_send.at[k], chain_recv.at[k], chain_s.at[k], chain_r.at[k],
            first_axis(half)[0], sign,
        )

    def chain_step(half, step):
        for part in range(2):
            for sign, hops in ((1, 4 - part), (-1, 3 + part)):
                if step >= hops:
                    continue
                k = CHAIN_AT[half, part, sign, step]
                to = lax.rem(first_axis(half)[1] + sign * (hops - step) + RING, RING)
                if step:
                    chain_copy(k - 1).wait_recv()
                at = 0
                for row, size in pieces(half, to, part):
                    value = partial[half, pl.ds(pl.multiple_of(row, size), size), :]
                    if step:
                        value = value + chain_recv[k - 1, at : at + size, :].astype(F32)
                    chain_send[k, at : at + size, :] = value.astype(BF16)
                    at += size
                chain_copy(k).start()

    def chain_end(half):
        for part in range(2):
            ends = [
                CHAIN_AT[half, part, sign, hops - 1]
                for sign, hops in ((1, 4 - part), (-1, 3 + part))
            ]
            for k in ends:
                chain_copy(k).wait_recv()
            at = 0
            for row, size in pieces(half, first_axis(half)[1], part):
                value = partial[half, pl.ds(pl.multiple_of(row, size), size), :]
                for k in ends:
                    value = value + chain_recv[k, at : at + size, :].astype(F32)
                for sub in range(size // ROWS):
                    slot = (part * 128 + at) // ROWS + sub
                    piece = value[sub * ROWS : (sub + 1) * ROWS]
                    summed[half, slot] = piece
                    cross_send[half, slot] = piece.astype(BF16)
                at += size

    def slot_of(half, at):
        return lax.rem(at, 4) * 2 + at // 4 if half == 0 else at

    def cross_copy(half, shift):
        axis, here = ("z", z) if half == 0 else ("y", y)
        slot = slot_of(half, lax.rem(here + shift, RING))
        return remote(
            cross_send.at[half, slot], cross_recv.at[half, shift],
            cross_s.at[half, shift], cross_r.at[half, shift], axis, shift,
        )

    def cross_start(half):
        for shift in FAR_FIRST:
            cross_copy(half, shift).start()

    def cross_end(half):
        here = z if half == 0 else y
        value = summed[half, slot_of(half, here)]
        for shift in FAR_FIRST:
            cross_copy(half, shift).wait_recv()
        for shift in FAR_FIRST:
            value = value + cross_recv[half, shift].astype(F32)
        final[:, half * HALF : (half + 1) * HALF] = value

    def swap_copy():
        return remote(final, other_final, swap_s.at[0], swap_r.at[0], "z", 4)

    def small_copies(kind, axis, src, dst):
        here = y if axis == "y" else z
        base = (kind * 2 + (axis == "z")) * RING
        size = 8 if kind == 0 else 1
        return [
            remote(
                src.at[pl.ds(0, size), :], dst.at[here, pl.ds(0, size), :],
                small_s.at[base + shift], small_r.at[base + shift], axis, shift,
            )
            for shift in FAR_FIRST
        ]

    def small_start(kind, axis, src, dst):
        here = y if axis == "y" else z
        size = 8 if kind == 0 else 1
        for copy in small_copies(kind, axis, src, dst):
            copy.start()
        dst[here, 0:size, :] = src[0:size, :]

    def small_end(kind, axis, src, dst):
        size = 8 if kind == 0 else 1
        for copy in small_copies(kind, axis, src, dst):
            copy.wait_recv()
        value = dst[0, 0:size, :]
        for k in range(1, RING):
            value = value + dst[k, 0:size, :]
        return value

    loads[0].wait()
    loads[1].wait()
    pl.semaphore_wait(barrier, 2 * (RING - 1))
    gather_round(0)
    loads[2].wait()
    loads[3].wait()
    forward(0)
    gather_round(1)
    loads[4].wait()
    weight_grad(0)
    chain_step(0, 0)
    gather_round(2)
    forward(1)
    weight_grad(1)
    chain_step(1, 0)
    gather_round(3)
    chain_step(0, 1)
    chain_step(1, 1)
    gather_round(4)
    chain_step(0, 2)
    chain_step(1, 2)
    gather_round(5)
    chain_step(0, 3)
    chain_step(1, 3)
    for number in range(6, LAST_ROUND + 2):
        gather_round(number)
    hidden_grad(0)
    chain_end(0)
    cross_start(0)
    chain_end(1)
    cross_start(1)
    hidden_grad(1)
    backward(0)
    backward(1)
    small_start(0, "y", conv_send, conv_y)
    stores = [
        pltpu.make_async_copy(gg, gg_hbm, store_sem.at[0]),
        pltpu.make_async_copy(gl, gl_hbm, store_sem.at[1]),
    ]
    for store in stores:
        store.start()
    cross_end(0)
    cross_end(1)
    swap_copy().start()
    norm_send[0:1, :] = jnp.sum(final[...] * final[...], axis=0, keepdims=True)
    small_start(1, "y", norm_send, norm_y)
    conv = small_end(0, "y", conv_send, conv_y)
    conv_send2 = conv_z.at[RING]
    conv_send2[...] = conv
    small_start(0, "z", conv_send2, conv_z)
    norm = small_end(1, "y", norm_send, norm_y)
    norm_send2 = norm_z.at[RING]
    norm_send2[0:1, :] = norm
    small_start(1, "z", norm_send2, norm_z)
    conv = small_end(0, "z", conv_send2, conv_z)
    taps_g_out[...] = conv[0:3]
    taps_l_out[...] = conv[3:6]
    bias_g_out[...] = conv[6:7]
    bias_l_out[...] = conv[7:8]
    swap_copy().wait_recv()
    down_out[pl.ds(pl.multiple_of(rep * ROWS, ROWS), ROWS), :] = final[...]
    down_out[pl.ds(pl.multiple_of((1 - rep) * ROWS, ROWS), ROWS), :] = other_final[...]
    norms_out[...] = small_end(1, "z", norm_send2, norm_z)

    for k in range(len(GATHER)):
        gather_copy(k).wait_send()
    for k in range(len(CHAIN)):
        chain_copy(k).wait_send()
    for half in range(2):
        for shift in FAR_FIRST:
            cross_copy(half, shift).wait_send()
    swap_copy().wait_send()
    for kind, axis, src, dst in (
        (0, "y", conv_send, conv_y), (0, "z", conv_send2, conv_z),
        (1, "y", norm_send, norm_y), (1, "z", norm_send2, norm_z),
    ):
        for copy in small_copies(kind, axis, src, dst):
            copy.wait_send()
    for store in stores:
        store.wait()


def local(
    pre_gate, pre_linear, taps_gate, taps_linear, bias_gate, bias_linear, down_weight, out_grad
):
    tokens, width = pre_gate.shape
    columns = out_grad.shape[1]
    any_, vmem = pl.BlockSpec(memory_space=pl.ANY), pl.BlockSpec(memory_space=pltpu.VMEM)
    dma = pltpu.SemaphoreType.DMA
    shape = jax.ShapeDtypeStruct
    out = pl.pallas_call(
        kernel,
        name="gated_backward",
        out_shape=(
            shape((tokens, width), BF16), shape((tokens, width), BF16),
            shape((3, width), F32), shape((3, width), F32),
            shape((1, width), F32), shape((1, width), F32),
            shape((BLOCK, width), F32), shape((1, width), F32),
        ),
        in_specs=[any_, any_, vmem, vmem, vmem, vmem, any_, any_],
        out_specs=(any_, any_, vmem, vmem, vmem, vmem, vmem, vmem),
        scratch_shapes=[
            pltpu.VMEM((tokens + 16, width), BF16),
            pltpu.VMEM((tokens + 16, width), BF16),
            pltpu.VMEM((tokens, columns), BF16),
            pltpu.VMEM((2, columns, HALF), BF16),
            pltpu.VMEM((tokens, width), BF16),
            pltpu.VMEM((tokens, width), F32),
            pltpu.VMEM((tokens, width), F32),
            pltpu.VMEM((tokens, width), F32),
            pltpu.VMEM((2, columns, HALF), F32),
            pltpu.VMEM((tokens, width), BF16),
            pltpu.VMEM((tokens, width), BF16),
            pltpu.VMEM((len(CHAIN), 128, HALF), BF16),
            pltpu.VMEM((len(CHAIN), 128, HALF), BF16),
            pltpu.VMEM((2, RING, ROWS, HALF), F32),
            pltpu.VMEM((2, RING, ROWS, HALF), BF16),
            pltpu.VMEM((2, RING, ROWS, HALF), BF16),
            pltpu.VMEM((ROWS, width), F32),
            pltpu.VMEM((ROWS, width), F32),
            pltpu.VMEM((8, width), F32),
            pltpu.VMEM((RING, 8, width), F32),
            pltpu.VMEM((RING + 1, 8, width), F32),
            pltpu.VMEM((8, width), F32),
            pltpu.VMEM((RING, 8, width), F32),
            pltpu.VMEM((RING + 1, 8, width), F32),
            dma((5,)), dma((2,)),
            dma((len(GATHER),)), dma((len(GATHER),)),
            dma((len(CHAIN),)), dma((len(CHAIN),)),
            dma((2, RING)), dma((2, RING)),
            dma((4 * RING,)), dma((4 * RING,)),
            dma((1,)), dma((1,)),
        ],
        compiler_params=pltpu.CompilerParams(
            collective_id=0, has_side_effects=True, vmem_limit_bytes=60 * 2**20
        ),
    )(
        pre_gate, pre_linear, taps_gate, taps_linear,
        bias_gate.reshape(1, -1), bias_linear.reshape(1, -1), down_weight.T, out_grad,
    )
    gg, gl, tg, tl, bg, bl, down, norms = out
    return gg, gl, tg, tl, bg.reshape(-1), bl.reshape(-1), down.T, norms.reshape(-1)


def solution(mesh):
    split = Mesh(
        mesh.devices.reshape(mesh.shape["rep"], 4, 8, mesh.shape["tp"]),
        ("rep", "fs_0", "fs_1", "tp"),
    )
    fs = ("fs_0", "fs_1")
    in_specs = (
        P(REP_FS, "tp"), P(REP_FS, "tp"), P(None, "tp"), P(None, "tp"),
        P("tp"), P("tp"), P("tp", fs), P(REP_FS, None),
    )
    out_specs = (
        P(REP_FS, "tp"), P(REP_FS, "tp"), P(None, "tp"), P(None, "tp"),
        P("tp"), P("tp"), P("tp", fs), P("tp"),
    )
    return jax.shard_map(local, mesh=split, in_specs=in_specs, out_specs=out_specs, check_vma=False)
```

```python
import jax
import jax.numpy as jnp
from jax import lax
from jax.experimental import pallas as pl
from jax.experimental.pallas import tpu as pltpu
from jax.sharding import Mesh
from jax.sharding import PartitionSpec as P

REP_FS = ("rep", "fs_0", "fs_1")
RING = 8
BLOCK = 64
HALF = 256
ROWS = 32
F32, BF16 = jnp.float32, jnp.bfloat16
FAR_FIRST = (4, 3, 5, 2, 6, 1, 7)


def gather_messages():
    found = []

    def add(half, dz, dy, part, axis, sign, needs):
        found.append((half, dz, dy, part, axis, sign, needs))
        return len(found) - 1

    right = add(0, 0, 0, 0, "z", 1, ())
    left = add(0, 0, 0, 0, "z", -1, ())
    right2 = add(0, -1, 0, 1, "z", 1, (right,))
    left2 = add(0, 1, 0, 2, "z", -1, (left,))
    for j, (dz, needs) in enumerate(
        ((0, ()), (-1, (right,)), (1, (left,)), (2, (right2, left2)))
    ):
        for sign, hops in ((1, 4 - j % 2), (-1, 3 + j % 2)):
            before = needs
            for k in range(hops):
                before = (add(0, dz, -sign * k, 0, "y", sign, before),)
    items = [(0, ())]
    for sign, hops in ((1, 4), (-1, 3)):
        before = ()
        for k in range(hops):
            before = (add(1, 0, -sign * k, 0, "y", sign, before),)
            items.append((-sign * (k + 1), before))
    for i, (dy, needs) in enumerate(items):
        first = add(1, 0, dy, 0, "z", 1, needs)
        other = add(1, 0, dy, 0, "z", -1, needs)
        if i % 2 == 0:
            add(1, -1, dy, 0, "z", 1, (first,))
        else:
            add(1, 1, dy, 0, "z", -1, (other,))
    return found


GATHER = gather_messages()
ROUND = []
for _m in GATHER:
    ROUND.append(1 + max((ROUND[k] for k in _m[6]), default=-1))
LAST_ROUND = max(ROUND)


def chain_messages():
    return [
        (half, part, sign, step, hops)
        for half in range(2)
        for part in range(2)
        for sign, hops in ((1, 4 - part), (-1, 3 + part))
        for step in range(hops)
    ]


CHAIN = chain_messages()
CHAIN_AT = {m[:4]: k for k, m in enumerate(CHAIN)}


def kernel(
    gate_hbm, linear_hbm, taps_g_hbm, taps_l_hbm, bias_g_hbm, bias_l_hbm, weight_hbm,
    out_grad_hbm,
    gg, gl, conv_out, down_out, norms_out,
    gate, linear, taps_g, taps_l, bias_g, bias_l, out_grad, weights, hidden, factor_g, factor_l, grad_hidden, partial,
    chain_send, chain_recv, summed, cross_send, cross_recv, final, other_final,
    conv_send, conv_y, conv_z, norm_send, norm_y, norm_z,
    load_sem, gather_s, gather_r, chain_s, chain_r, cross_s, cross_r,
    small_s, small_r, swap_s, swap_r,
):
    tokens = gate_hbm.shape[0]
    rep, z_lo, y = lax.axis_index("rep"), lax.axis_index("fs_0"), lax.axis_index("fs_1")
    z = rep * 4 + z_lo

    def along(axis, shift):
        if axis == "y":
            return {"fs_1": lax.rem(y + shift + RING, RING)}
        at = lax.rem(z + shift + RING, RING)
        return {"rep": at // 4, "fs_0": lax.rem(at, 4)}

    def remote(src, dst, send, recv, axis, shift):
        return pltpu.make_async_remote_copy(
            src_ref=src, dst_ref=dst, send_sem=send, recv_sem=recv,
            device_id=along(axis, shift), device_id_type=pl.DeviceIdType.MESH,
        )

    barrier = pltpu.get_barrier_semaphore()
    for axis in ("y", "z"):
        for shift in range(1, RING):
            pl.semaphore_signal(
                barrier, inc=1, device_id=along(axis, shift),
                device_id_type=pl.DeviceIdType.MESH,
            )

    own_row = pl.multiple_of((z_lo * 8 + y) * BLOCK, BLOCK)
    loads = [
        pltpu.make_async_copy(
            weight_hbm.at[:, pl.ds(h * HALF, HALF)],
            weights.at[h, pl.ds(own_row, BLOCK), :],
            load_sem.at[h],
        )
        for h in range(2)
    ]
    loads += [
        pltpu.make_async_copy(gate_hbm, gate.at[pl.ds(16, tokens), :], load_sem.at[2]),
        pltpu.make_async_copy(linear_hbm, linear.at[pl.ds(16, tokens), :], load_sem.at[3]),
        pltpu.make_async_copy(taps_g_hbm, taps_g, load_sem.at[5]),
        pltpu.make_async_copy(taps_l_hbm, taps_l, load_sem.at[6]),
        pltpu.make_async_copy(bias_g_hbm, bias_g, load_sem.at[7]),
        pltpu.make_async_copy(bias_l_hbm, bias_l, load_sem.at[8]),
        pltpu.make_async_copy(out_grad_hbm, out_grad, load_sem.at[4]),
    ]
    for load in loads:
        load.start()
    for ref in (gate, linear):
        ref[0:16, :] = jnp.zeros((16, ref.shape[1]), BF16)

    def gather_copy(k):
        half, dz, dy, part, axis, sign, _ = GATHER[k]
        at = lax.rem(z_lo + dz + 4, 4) * 8 + lax.rem(y + dy + RING, RING)
        start, size = at * BLOCK, BLOCK
        if part:
            start, size = start + (part - 1) * 32, 32
        block = weights.at[half, pl.ds(pl.multiple_of(start, size), size), :]
        return remote(block, block, gather_s.at[k], gather_r.at[k], axis, sign)

    def gather_round(number):
        arrived = set(k for k, r in enumerate(ROUND) if r < number - 1)
        todo = [k for k, r in enumerate(ROUND) if r == number]
        for k in [k for k, r in enumerate(ROUND) if r == number - 1]:
            gather_copy(k).wait_recv()
            arrived.add(k)
            for m in list(todo):
                if all(n in arrived for n in GATHER[m][6]):
                    gather_copy(m).start()
                    todo.remove(m)
        for m in todo:
            gather_copy(m).start()

    STEP = 32

    def shifted(ref, row, lanes):
        rows = ref[pl.ds(row, STEP + 16), lanes].astype(F32)
        return pltpu.roll(rows, 2, 0)[16:], pltpu.roll(rows, 1, 0)[16:], rows[16:]

    def forward(half):
        lanes = slice(half * HALF, (half + 1) * HALF)
        tg, tl = taps_g[0:3, lanes], taps_l[0:3, lanes]
        bg, bl = bias_g[0:1, lanes], bias_l[0:1, lanes]

        def body(i, carry):
            row = pl.multiple_of(i * STEP, STEP)
            g0, g1, g2 = shifted(gate, row, lanes)
            l0, l1, l2 = shifted(linear, row, lanes)
            gate_pre = tg[0:1] * g0 + tg[1:2] * g1 + tg[2:3] * g2 + bg
            linear_pre = tl[0:1] * l0 + tl[1:2] * l1 + tl[2:3] * l2 + bl
            sigma = 1.0 / (1.0 + jnp.exp(-gate_pre))
            silu = gate_pre * sigma
            hidden[pl.ds(row, STEP), lanes] = (silu * linear_pre).astype(BF16)
            factor_g[pl.ds(row, STEP), lanes] = (
                linear_pre * sigma * (1.0 + gate_pre * (1.0 - sigma))
            )
            factor_l[pl.ds(row, STEP), lanes] = silu
            return carry

        lax.fori_loop(0, tokens // STEP, body, 0)

    def weight_grad(half):
        lanes = slice(half * HALF, (half + 1) * HALF)

        def body(i, carry):
            at = pl.multiple_of(i * 512, 512)
            partial[half, pl.ds(at, 512), :] = lax.dot_general(
                out_grad[:, pl.ds(at, 512)], hidden[:, lanes],
                (((0,), (0,)), ((), ())), preferred_element_type=F32,
            )
            return carry

        lax.fori_loop(0, 4, body, 0)

    def hidden_grad(half):
        lanes = slice(half * HALF, (half + 1) * HALF)

        def body(i, carry):
            at = pl.multiple_of(i * 256, 256)
            grad_hidden[pl.ds(at, 256), lanes] = jnp.dot(
                out_grad[pl.ds(at, 256), :], weights[half], preferred_element_type=F32
            )
            return carry

        lax.fori_loop(0, tokens // 256, body, 0)

    def fold(v):
        return jnp.sum(v.reshape(STEP // 8, 8, HALF), axis=0)

    def backward(half):
        lanes = slice(half * HALF, (half + 1) * HALF)
        tg, tl = taps_g[0:3, lanes], taps_l[0:3, lanes]

        def back(v, after, taps):
            longer = jnp.concatenate([v, after], axis=0)
            one = pltpu.roll(longer, STEP + 7, 0)[0:STEP]
            two = pltpu.roll(longer, STEP + 6, 0)[0:STEP]
            return taps[0:1] * two + taps[1:2] * one + taps[2:3] * v

        def body(i, carry):
            after_g, after_l, sums = carry
            row = pl.multiple_of((tokens // STEP - 1 - i) * STEP, STEP)
            grad = grad_hidden[pl.ds(row, STEP), lanes]
            dg = grad * factor_g[pl.ds(row, STEP), lanes]
            dl = grad * factor_l[pl.ds(row, STEP), lanes]
            gs = shifted(gate, row, lanes)
            ls = shifted(linear, row, lanes)
            gg[pl.ds(row, STEP), lanes] = back(dg, after_g, tg).astype(BF16)
            gl[pl.ds(row, STEP), lanes] = back(dl, after_l, tl).astype(BF16)
            terms = [dg * v for v in gs] + [dl * v for v in ls] + [dg, dl]
            sums = tuple(s + fold(t) for s, t in zip(sums, terms))
            return dg[0:8], dl[0:8], sums

        zero = jnp.zeros((8, HALF), F32)
        _, _, sums = lax.fori_loop(0, tokens // STEP, body, (zero, zero, (zero,) * 8))
        for j, s in enumerate(sums):
            conv_send[j : j + 1, lanes] = jnp.sum(s, axis=0, keepdims=True)

    def first_axis(half):
        return ("y", y) if half == 0 else ("z", z)

    def pieces(half, to, part):
        if half == 0:
            return [((2 * part + q) * 512 + to * 64, 64) for q in range(2)]
        return [
            (lax.rem(to, 4) * 512 + (4 * part + q) * 64 + (to // 4) * 32, 32)
            for q in range(4)
        ]

    def chain_copy(k):
        half, part, sign, step, hops = CHAIN[k]
        return remote(
            chain_send.at[k], chain_recv.at[k], chain_s.at[k], chain_r.at[k],
            first_axis(half)[0], sign,
        )

    def chain_step(half, step):
        for part in range(2):
            for sign, hops in ((1, 4 - part), (-1, 3 + part)):
                if step >= hops:
                    continue
                k = CHAIN_AT[half, part, sign, step]
                to = lax.rem(first_axis(half)[1] + sign * (hops - step) + RING, RING)
                if step:
                    chain_copy(k - 1).wait_recv()
                at = 0
                for row, size in pieces(half, to, part):
                    value = partial[half, pl.ds(pl.multiple_of(row, size), size), :]
                    if step:
                        value = value + chain_recv[k - 1, at : at + size, :].astype(F32)
                    chain_send[k, at : at + size, :] = value.astype(BF16)
                    at += size
                chain_copy(k).start()

    def chain_end(half):
        for part in range(2):
            ends = [
                CHAIN_AT[half, part, sign, hops - 1]
                for sign, hops in ((1, 4 - part), (-1, 3 + part))
            ]
            for k in ends:
                chain_copy(k).wait_recv()
            at = 0
            for row, size in pieces(half, first_axis(half)[1], part):
                value = partial[half, pl.ds(pl.multiple_of(row, size), size), :]
                for k in ends:
                    value = value + chain_recv[k, at : at + size, :].astype(F32)
                for sub in range(size // ROWS):
                    slot = (part * 128 + at) // ROWS + sub
                    piece = value[sub * ROWS : (sub + 1) * ROWS]
                    summed[half, slot] = piece
                    cross_send[half, slot] = piece.astype(BF16)
                at += size

    def slot_of(half, at):
        return lax.rem(at, 4) * 2 + at // 4 if half == 0 else at

    def cross_copy(half, shift):
        axis, here = ("z", z) if half == 0 else ("y", y)
        slot = slot_of(half, lax.rem(here + shift, RING))
        return remote(
            cross_send.at[half, slot], cross_recv.at[half, shift],
            cross_s.at[half, shift], cross_r.at[half, shift], axis, shift,
        )

    def cross_start(half):
        for shift in FAR_FIRST:
            cross_copy(half, shift).start()

    def cross_end(half):
        here = z if half == 0 else y
        value = summed[half, slot_of(half, here)]
        for shift in FAR_FIRST:
            cross_copy(half, shift).wait_recv()
        for shift in FAR_FIRST:
            value = value + cross_recv[half, shift].astype(F32)
        final[:, half * HALF : (half + 1) * HALF] = value

    def swap_copy():
        return remote(final, other_final, swap_s.at[0], swap_r.at[0], "z", 4)

    def small_copies(kind, axis, src, dst):
        here = y if axis == "y" else z
        base = (kind * 2 + (axis == "z")) * RING
        size = 8 if kind == 0 else 1
        return [
            remote(
                src.at[pl.ds(0, size), :], dst.at[here, pl.ds(0, size), :],
                small_s.at[base + shift], small_r.at[base + shift], axis, shift,
            )
            for shift in FAR_FIRST
        ]

    def small_start(kind, axis, src, dst):
        here = y if axis == "y" else z
        size = 8 if kind == 0 else 1
        for copy in small_copies(kind, axis, src, dst):
            copy.start()
        dst[here, 0:size, :] = src[0:size, :]

    def small_end(kind, axis, src, dst):
        size = 8 if kind == 0 else 1
        for copy in small_copies(kind, axis, src, dst):
            copy.wait_recv()
        value = dst[0, 0:size, :]
        for k in range(1, RING):
            value = value + dst[k, 0:size, :]
        return value

    loads[0].wait()
    loads[1].wait()
    pl.semaphore_wait(barrier, 2 * (RING - 1))
    gather_round(0)
    for load in loads[2:8]:
        load.wait()
    forward(0)
    gather_round(1)
    loads[8].wait()
    weight_grad(0)
    chain_step(0, 0)
    gather_round(2)
    forward(1)
    weight_grad(1)
    chain_step(1, 0)
    gather_round(3)
    chain_step(0, 1)
    chain_step(1, 1)
    gather_round(4)
    chain_step(0, 2)
    chain_step(1, 2)
    gather_round(5)
    chain_step(0, 3)
    chain_step(1, 3)
    for number in range(6, LAST_ROUND + 2):
        gather_round(number)
    hidden_grad(0)
    chain_end(0)
    cross_start(0)
    chain_end(1)
    cross_start(1)
    hidden_grad(1)
    backward(0)
    backward(1)
    small_start(0, "y", conv_send, conv_y)
    cross_end(0)
    cross_end(1)
    swap_copy().start()
    norm_send[0:1, :] = jnp.sum(final[...] * final[...], axis=0, keepdims=True)
    small_start(1, "y", norm_send, norm_y)
    conv = small_end(0, "y", conv_send, conv_y)
    conv_send2 = conv_z.at[RING]
    conv_send2[...] = conv
    small_start(0, "z", conv_send2, conv_z)
    norm = small_end(1, "y", norm_send, norm_y)
    norm_send2 = norm_z.at[RING]
    norm_send2[0:1, :] = norm
    small_start(1, "z", norm_send2, norm_z)
    conv_out[...] = small_end(0, "z", conv_send2, conv_z)
    swap_copy().wait_recv()
    down_out[pl.ds(pl.multiple_of(rep * ROWS, ROWS), ROWS), :] = final[...]
    down_out[pl.ds(pl.multiple_of((1 - rep) * ROWS, ROWS), ROWS), :] = other_final[...]
    norms_out[...] = small_end(1, "z", norm_send2, norm_z)

    for k in range(len(GATHER)):
        gather_copy(k).wait_send()
    for k in range(len(CHAIN)):
        chain_copy(k).wait_send()
    for half in range(2):
        for shift in FAR_FIRST:
            cross_copy(half, shift).wait_send()
    swap_copy().wait_send()
    for kind, axis, src, dst in (
        (0, "y", conv_send, conv_y), (0, "z", conv_send2, conv_z),
        (1, "y", norm_send, norm_y), (1, "z", norm_send2, norm_z),
    ):
        for copy in small_copies(kind, axis, src, dst):
            copy.wait_send()


def in_hbm(array):
    return pltpu.with_memory_space_constraint(array, pltpu.HBM)


def finish(gg, gl, conv, down, norms, gg_o, gl_o, tg_o, tl_o, bg_o, bl_o, down_o, norms_o, sems):
    moves = (
        (gg, gg_o), (gl, gl_o), (conv.at[pl.ds(0, 3), :], tg_o), (conv.at[pl.ds(3, 3), :], tl_o),
        (conv.at[pl.ds(6, 1), :], bg_o), (conv.at[pl.ds(7, 1), :], bl_o),
        (down, down_o), (norms, norms_o),
    )
    copies = [pltpu.make_async_copy(a, b, sems.at[k]) for k, (a, b) in enumerate(moves)]
    for copy in copies:
        copy.start()
    for copy in copies:
        copy.wait()


def local(
    pre_gate, pre_linear, taps_gate, taps_linear, bias_gate, bias_linear, down_weight, out_grad
):
    tokens, width = pre_gate.shape
    columns = out_grad.shape[1]
    any_, vmem = pl.BlockSpec(memory_space=pl.ANY), pl.BlockSpec(memory_space=pltpu.VMEM)
    hbm = pl.BlockSpec(memory_space=pltpu.HBM)
    dma = pltpu.SemaphoreType.DMA
    shape = jax.ShapeDtypeStruct
    held = pl.pallas_call(
        kernel,
        name="gated_backward",
        out_shape=(
            pltpu.VMEM((tokens, width), BF16), pltpu.VMEM((tokens, width), BF16),
            pltpu.VMEM((8, width), F32), pltpu.VMEM((BLOCK, width), F32),
            pltpu.VMEM((1, width), F32),
        ),
        in_specs=[hbm] * 8,
        out_specs=(vmem,) * 5,
        scratch_shapes=[
            pltpu.VMEM((tokens + 16, width), BF16),
            pltpu.VMEM((tokens + 16, width), BF16),
            pltpu.VMEM((3, width), F32),
            pltpu.VMEM((3, width), F32),
            pltpu.VMEM((1, width), F32),
            pltpu.VMEM((1, width), F32),
            pltpu.VMEM((tokens, columns), BF16),
            pltpu.VMEM((2, columns, HALF), BF16),
            pltpu.VMEM((tokens, width), BF16),
            pltpu.VMEM((tokens, width), F32),
            pltpu.VMEM((tokens, width), F32),
            pltpu.VMEM((tokens, width), F32),
            pltpu.VMEM((2, columns, HALF), F32),
            pltpu.VMEM((len(CHAIN), 128, HALF), BF16),
            pltpu.VMEM((len(CHAIN), 128, HALF), BF16),
            pltpu.VMEM((2, RING, ROWS, HALF), F32),
            pltpu.VMEM((2, RING, ROWS, HALF), BF16),
            pltpu.VMEM((2, RING, ROWS, HALF), BF16),
            pltpu.VMEM((ROWS, width), F32),
            pltpu.VMEM((ROWS, width), F32),
            pltpu.VMEM((8, width), F32),
            pltpu.VMEM((RING, 8, width), F32),
            pltpu.VMEM((RING + 1, 8, width), F32),
            pltpu.VMEM((8, width), F32),
            pltpu.VMEM((RING, 8, width), F32),
            pltpu.VMEM((RING + 1, 8, width), F32),
            dma((9,)),
            dma((len(GATHER),)), dma((len(GATHER),)),
            dma((len(CHAIN),)), dma((len(CHAIN),)),
            dma((2, RING)), dma((2, RING)),
            dma((4 * RING,)), dma((4 * RING,)),
            dma((1,)), dma((1,)),
        ],
        compiler_params=pltpu.CompilerParams(
            collective_id=0, has_side_effects=True, vmem_limit_bytes=40 * 2**20
        ),
    )(
        *map(
            in_hbm,
            (
                pre_gate, pre_linear, taps_gate, taps_linear, bias_gate.reshape(1, -1),
                bias_linear.reshape(1, -1), down_weight.T, out_grad,
            ),
        )
    )
    gg, gl, tg, tl, bg, bl, down, norms = pl.pallas_call(
        finish,
        name="finish",
        out_shape=(
            shape((tokens, width), BF16), shape((tokens, width), BF16),
            shape((3, width), F32), shape((3, width), F32),
            shape((1, width), F32), shape((1, width), F32),
            shape((BLOCK, width), F32), shape((1, width), F32),
        ),
        in_specs=[vmem] * 5,
        out_specs=(any_,) * 8,
        scratch_shapes=[dma((8,))],
        compiler_params=pltpu.CompilerParams(vmem_limit_bytes=8 * 2**20),
    )(*held)
    return gg, gl, tg, tl, bg.reshape(-1), bl.reshape(-1), down.T, norms.reshape(-1)


def solution(mesh):
    split = Mesh(
        mesh.devices.reshape(mesh.shape["rep"], 4, 8, mesh.shape["tp"]),
        ("rep", "fs_0", "fs_1", "tp"),
    )
    fs = ("fs_0", "fs_1")
    in_specs = (
        P(REP_FS, "tp"), P(REP_FS, "tp"), P(None, "tp"), P(None, "tp"),
        P("tp"), P("tp"), P("tp", fs), P(REP_FS, None),
    )
    out_specs = (
        P(REP_FS, "tp"), P(REP_FS, "tp"), P(None, "tp"), P(None, "tp"),
        P("tp"), P("tp"), P("tp", fs), P("tp"),
    )
    return jax.shard_map(local, mesh=split, in_specs=in_specs, out_specs=out_specs, check_vma=False)
```

```python
import jax
import jax.numpy as jnp
from jax import lax
from jax.experimental import pallas as pl
from jax.experimental.pallas import tpu as pltpu
from jax.sharding import Mesh
from jax.sharding import PartitionSpec as P

REP_FS = ("rep", "fs_0", "fs_1")
RING = 8
BLOCK = 64
HALF = 256
LANES = 128
ROWS = 32
F32, BF16 = jnp.float32, jnp.bfloat16
FAR_FIRST = (4, 3, 5, 2, 6, 1, 7)


def gather_messages():
    found = []

    def add(half, dz, dy, part, axis, sign, needs):
        found.append((half, dz, dy, part, axis, sign, needs))
        return len(found) - 1

    right = add(0, 0, 0, 0, "z", 1, ())
    left = add(0, 0, 0, 0, "z", -1, ())
    right2 = add(0, -1, 0, 1, "z", 1, (right,))
    left2 = add(0, 1, 0, 2, "z", -1, (left,))
    for j, (dz, needs) in enumerate(
        ((0, ()), (-1, (right,)), (1, (left,)), (2, (right2, left2)))
    ):
        for sign, hops in ((1, 4 - j % 2), (-1, 3 + j % 2)):
            before = needs
            for k in range(hops):
                before = (add(0, dz, -sign * k, 0, "y", sign, before),)
    items = [(0, ())]
    for sign, hops in ((1, 4), (-1, 3)):
        before = ()
        for k in range(hops):
            before = (add(1, 0, -sign * k, 0, "y", sign, before),)
            items.append((-sign * (k + 1), before))
    for i, (dy, needs) in enumerate(items):
        first = add(1, 0, dy, 0, "z", 1, needs)
        other = add(1, 0, dy, 0, "z", -1, needs)
        if i % 2 == 0:
            add(1, -1, dy, 0, "z", 1, (first,))
        else:
            add(1, 1, dy, 0, "z", -1, (other,))
    return found


PARTS = 4


def chain_messages():
    return [
        (half, part, sign, step, hops)
        for half in range(2)
        for part in range(PARTS)
        for sign, hops in ((1, 4 - part % 2), (-1, 3 + part % 2))
        for step in range(hops)
    ]


GATHER = gather_messages()
CHAIN = chain_messages()
CHAIN_AT = {m[:4]: k for k, m in enumerate(CHAIN)}


def chain_ends(half, part):
    return [
        CHAIN_AT[half, part, sign, hops - 1]
        for sign, hops in ((1, 4 - part % 2), (-1, 3 + part % 2))
    ]


RATE, FIRST_HOP, NEXT_HOP, BACKLOG = 44.4, 2.1, 0.8, 1.5


def steps():
    found = {}

    def step(name, time, rank, after=(), needs=(), sends=(), start=0.0):
        found[name] = (time, rank, start, tuple(after), tuple(needs), tuple(sends))

    def to_all(kind, half, axis, size):
        return [
            ((kind, half, shift), axis, 1 if shift < 4 + (half == 0) else -1, size,
             min(shift, RING - shift))
            for shift in FAR_FIRST
        ]

    follow = [1] * len(GATHER)
    for k in reversed(range(len(GATHER))):
        for n in GATHER[k][6]:
            follow[n] = max(follow[n], follow[k] + 1)
    for k, (half, _, _, part, axis, sign, needs) in enumerate(GATHER):
        step(("g", k), 0.04, 0.3 - 0.01 * follow[k], (), [("g", n) for n in needs],
             [(("g", k), axis, sign, 16 if part else 32, 1)], 1.0)
    for half in range(2):
        first, second = ("y", "z") if half == 0 else ("z", "y")
        for i in range(2):
            step(("f", half, i), 0.5, 3 + half, [("f", half, 0)] * i, start=2.0)
        for i in range(4):
            before = [("f", half, 1)] + [("w", half, i - 1)] * (i > 0)
            step(("w", half, i), 0.38, 2.5 + half, before, start=2.5)
        for k, (h, part, sign, at, hops) in enumerate(CHAIN):
            if h == half:
                ready = ("w", half, part if half == 0 else 3)
                step(("c", k), 0.07, 0.6 - 0.01 * (hops - at) - 0.1 * half, [ready],
                     [("c", k - 1)] * (at > 0), [(("c", k), first, sign, 128 // PARTS, 1)])
        ends = [("c", k) for part in range(PARTS) for k in chain_ends(half, part)]
        step(("ce", half), 0.25, 0.2, [("w", half, 3)], ends)
        step(("xs", half), 0.02, 0.1, [("ce", 0), ("ce", 1)], (), to_all("x", half, second, 16))
        step(("xe", half), 0.15, 0.1, [("xs", half)], [("x", half, n) for n in FAR_FIRST],
             to_all("ny", half, "y", 1))
        step(("ne", half), 0.1, 0.1, [("xe", half)], [("ny", half, n) for n in FAR_FIRST],
             to_all("nz", half, "z", 1))
        step(("no", half), 0.1, 0.1, [("ne", half)], [("nz", half, n) for n in FAR_FIRST])
        step(("ss", half), 0.02, 6, [("ne", half)], (),
             [(("s", half), "z", 1 if half else -1, 32, 4)])
        step(("so", half), 0.05, 6, [("ss", half)], [("s", half)])
        every = [("g", k) for k, m in enumerate(GATHER) if m[0] == half]
        for i in range(3):
            before = [("h", half, i - 1)] if i else every
            step(("h", half, i), 0.3, 5, before, () if i else every)
            step(("b", half, i), 0.45, 5, [("h", half, i)] + [("b", half, i - 1)] * (i > 0), (),
                 to_all("vy", half, "y", 8) if i == 2 else ())
        step(("ve", half), 0.1, 0.2, [("b", half, 2), ("ce", 1)],
             [("vy", half, n) for n in FAR_FIRST], to_all("vz", half, "z", 8))
        step(("vo", half), 0.1, 0.2, [("ve", half)], [("vz", half, n) for n in FAR_FIRST])
    return found


def planned():
    left = steps()
    clock, order, done, arrival = 0.0, [], set(), {}
    free = {(axis, sign): 0.0 for axis in "yz" for sign in (1, -1)}
    while left:
        choices = []
        for name, (_, rank, start, after, needs, sends) in left.items():
            if all(n in done for n in after) and all(n in arrival for n in needs):
                at = max([start] + [arrival[n] for n in needs])
                if name[0] == "g":
                    at = max(at, free[sends[0][1:3]] - BACKLOG)
                choices.append((max(at - clock, 0.0), rank, at, name))
        wait, _, _, name = min(choices)
        time, sends = left[name][0], left[name][5]
        del left[name]
        clock += wait + time
        order.append(name)
        done.add(name)
        for message, axis, sign, size, hops in sends:
            gone = max(clock, free[axis, sign]) + size * hops / RATE
            free[axis, sign] = gone
            arrival[message] = gone + FIRST_HOP + NEXT_HOP * (hops - 1)
    return order


ORDER = planned()


def kernel(
    gate_hbm, linear_hbm, taps_g_hbm, taps_l_hbm, bias_g_hbm, bias_l_hbm, weight_hbm,
    out_grad_hbm,
    gg, gl, conv_out, down_out, norms_out,
    gate, linear, taps_g, taps_l, bias_g, bias_l, out_grad, weights, hidden, factor_g, factor_l, grad_hidden, partial,
    chain_send, chain_recv, summed, cross_send, cross_recv, final, other_final,
    rows_g, rows_l, after_g, after_l, sums, conv_y, conv_z, norm_y, norm_z,
    load_sem, gather_s, gather_r, chain_s, chain_r, cross_s, cross_r,
    small_s, small_r, swap_s, swap_r,
):
    tokens = gate_hbm.shape[0]
    rep, z_lo, y = lax.axis_index("rep"), lax.axis_index("fs_0"), lax.axis_index("fs_1")
    z = rep * 4 + z_lo

    def along(axis, shift):
        if axis == "y":
            return {"fs_1": lax.rem(y + shift + RING, RING)}
        at = lax.rem(z + shift + RING, RING)
        return {"rep": at // 4, "fs_0": lax.rem(at, 4)}

    def remote(src, dst, send, recv, axis, shift):
        return pltpu.make_async_remote_copy(
            src_ref=src, dst_ref=dst, send_sem=send, recv_sem=recv,
            device_id=along(axis, shift), device_id_type=pl.DeviceIdType.MESH,
        )

    barrier = pltpu.get_barrier_semaphore()
    for axis in ("y", "z"):
        for shift in (1, -1):
            pl.semaphore_signal(
                barrier, inc=1, device_id=along(axis, shift),
                device_id_type=pl.DeviceIdType.MESH,
            )

    own_row = pl.multiple_of((z_lo * 8 + y) * BLOCK, BLOCK)
    loads = [
        pltpu.make_async_copy(
            weight_hbm.at[:, pl.ds(h * HALF, HALF)],
            weights.at[h, pl.ds(own_row, BLOCK), :],
            load_sem.at[h],
        )
        for h in range(2)
    ]
    loads += [
        pltpu.make_async_copy(gate_hbm, gate, load_sem.at[2]),
        pltpu.make_async_copy(linear_hbm, linear, load_sem.at[3]),
        pltpu.make_async_copy(taps_g_hbm, taps_g, load_sem.at[5]),
        pltpu.make_async_copy(taps_l_hbm, taps_l, load_sem.at[6]),
        pltpu.make_async_copy(bias_g_hbm, bias_g, load_sem.at[7]),
        pltpu.make_async_copy(bias_l_hbm, bias_l, load_sem.at[8]),
        pltpu.make_async_copy(out_grad_hbm, out_grad, load_sem.at[4]),
    ]
    for load in loads:
        load.start()
    strips = rows_g.shape[0]
    for ref in (rows_g, rows_l):
        ref[:, 0:8, :] = jnp.zeros((strips, 8, LANES), F32)
    for ref in (after_g, after_l):
        ref[:, tokens : tokens + 8, :] = jnp.zeros((strips, 8, LANES), F32)

    def gather_copy(k):
        half, dz, dy, part, axis, sign, _ = GATHER[k]
        at = lax.rem(z_lo + dz + 4, 4) * 8 + lax.rem(y + dy + RING, RING)
        start, size = at * BLOCK, BLOCK
        if part:
            start, size = start + (part - 1) * 32, 32
        block = weights.at[half, pl.ds(pl.multiple_of(start, size), size), :]
        return remote(block, block, gather_s.at[k], gather_r.at[k], axis, sign)

    STEP = 64

    def strips_of(half):
        return [(n, slice(n * LANES, (n + 1) * LANES)) for n in (2 * half, 2 * half + 1)]

    def forward(half, seg):
        blocks = tokens // STEP // 2
        for n, lanes in strips_of(half):
            tg, tl = taps_g[0:3, lanes], taps_l[0:3, lanes]
            bg, bl = bias_g[0:1, lanes], bias_l[0:1, lanes]

            def convolve(source, rows, row, taps, bias):
                last = source[pl.ds(row, STEP), lanes].astype(F32)
                rows[n, pl.ds(row + 8, STEP), :] = last
                return (
                    taps[0:1] * rows[n, pl.ds(row + 6, STEP), :]
                    + taps[1:2] * rows[n, pl.ds(row + 7, STEP), :]
                    + taps[2:3] * last
                    + bias
                )

            def body(i, carry):
                row = pl.multiple_of(i * STEP, STEP)
                gate_pre = convolve(gate, rows_g, row, tg, bg)
                linear_pre = convolve(linear, rows_l, row, tl, bl)
                sigma = 1.0 / (1.0 + jnp.exp(-gate_pre))
                silu = gate_pre * sigma
                hidden[pl.ds(row, STEP), lanes] = (silu * linear_pre).astype(BF16)
                factor_g[pl.ds(row, STEP), lanes] = (
                    linear_pre * sigma * (1.0 + gate_pre * (1.0 - sigma))
                )
                factor_l[pl.ds(row, STEP), lanes] = silu
                return carry

            lax.fori_loop(seg * blocks, (seg + 1) * blocks, body, 0)

    def weight_grad(half, i):
        lanes = slice(half * HALF, (half + 1) * HALF)
        partial[half, i * 512 : (i + 1) * 512, :] = lax.dot_general(
            out_grad[:, i * 512 : (i + 1) * 512], hidden[:, lanes],
            (((0,), (0,)), ((), ())), preferred_element_type=F32,
        )

    def hidden_grad(half, i):
        at, size = (2 - i) * (tokens // 3), tokens // 3
        grad_hidden[at : at + size, half * HALF : (half + 1) * HALF] = jnp.dot(
            out_grad[at : at + size, :], weights[half], preferred_element_type=F32
        )

    def fold(v):
        return jnp.sum(v.reshape(STEP // 8, 8, LANES), axis=0)

    def backward(half, seg):
        blocks = tokens // STEP // 3
        for n, lanes in strips_of(half):
            tg, tl = taps_g[0:3, lanes], taps_l[0:3, lanes]

            def back(v, after, row, taps):
                after[n, pl.ds(row, STEP), :] = v
                return (
                    taps[0:1] * after[n, pl.ds(row + 2, STEP), :]
                    + taps[1:2] * after[n, pl.ds(row + 1, STEP), :]
                    + taps[2:3] * v
                )

            def body(i, totals):
                row = pl.multiple_of((tokens // STEP - 1 - i) * STEP, STEP)
                grad = grad_hidden[pl.ds(row, STEP), lanes]
                dg = grad * factor_g[pl.ds(row, STEP), lanes]
                dl = grad * factor_l[pl.ds(row, STEP), lanes]
                gg[pl.ds(row, STEP), lanes] = back(dg, after_g, row, tg).astype(BF16)
                gl[pl.ds(row, STEP), lanes] = back(dl, after_l, row, tl).astype(BF16)
                terms = [dg * rows_g[n, pl.ds(row + 6 + j, STEP), :] for j in range(3)]
                terms += [dl * rows_l[n, pl.ds(row + 6 + j, STEP), :] for j in range(3)]
                terms += [dg, dl]
                return tuple(total + fold(term) for total, term in zip(totals, terms))

            if seg == 0:
                totals = (jnp.zeros((8, LANES), F32),) * 8
            else:
                totals = tuple(sums[j, :, lanes] for j in range(8))
            totals = lax.fori_loop(seg * blocks, (seg + 1) * blocks, body, totals)
            for j, total in enumerate(totals):
                sums[j, :, lanes] = total
        if seg == 2:
            for n, lanes in strips_of(half):
                for j in range(8):
                    total = jnp.sum(sums[j, :, lanes], axis=0, keepdims=True)
                    at = (n - 2 * half) * LANES
                    conv_y[half, RING, j : j + 1, at : at + LANES] = total
            small_start(0, half, "y", conv_y)

    def first_axis(half):
        return ("y", y) if half == 0 else ("z", z)

    def pieces(half, to, part):
        if half == 0:
            return [(part * 512 + to * 64, 64)]
        return [
            (lax.rem(to, 4) * 512 + (2 * part + q) * 64 + (to // 4) * 32, 32) for q in range(2)
        ]

    def chain_copy(k):
        half, part, sign, step, hops = CHAIN[k]
        return remote(
            chain_send.at[k], chain_recv.at[k], chain_s.at[k], chain_r.at[k],
            first_axis(half)[0], sign,
        )

    def chain_step(k):
        half, part, sign, step, hops = CHAIN[k]
        to = lax.rem(first_axis(half)[1] + sign * (hops - step) + RING, RING)
        at = 0
        for row, size in pieces(half, to, part):
            value = partial[half, pl.ds(pl.multiple_of(row, size), size), :]
            if step:
                value = value + chain_recv[k - 1, at : at + size, :].astype(F32)
            chain_send[k, at : at + size, :] = value.astype(BF16)
            at += size
        chain_copy(k).start()

    def chain_end(half):
        for part in range(PARTS):
            at = 0
            for row, size in pieces(half, first_axis(half)[1], part):
                value = partial[half, pl.ds(pl.multiple_of(row, size), size), :]
                for k in chain_ends(half, part):
                    value = value + chain_recv[k, at : at + size, :].astype(F32)
                for sub in range(size // ROWS):
                    slot = (part * BLOCK + at) // ROWS + sub
                    piece = value[sub * ROWS : (sub + 1) * ROWS]
                    summed[half, slot] = piece
                    cross_send[half, slot] = piece.astype(BF16)
                at += size

    def slot_of(half, at):
        return lax.rem(at, 4) * 2 + at // 4 if half == 0 else at

    def cross_copy(half, shift):
        axis, here = ("z", z) if half == 0 else ("y", y)
        slot = slot_of(half, lax.rem(here + shift, RING))
        return remote(
            cross_send.at[half, slot], cross_recv.at[half, shift],
            cross_s.at[half, shift], cross_r.at[half, shift], axis, shift,
        )

    def cross_start(half):
        for shift in FAR_FIRST:
            cross_copy(half, shift).start()

    def cross_end(half):
        here = z if half == 0 else y
        value = summed[half, slot_of(half, here)]
        for shift in FAR_FIRST:
            value = value + cross_recv[half, shift].astype(F32)
        final[half] = value
        norm_y[half, RING, 0:1, :] = jnp.sum(value * value, axis=0, keepdims=True)
        small_start(1, half, "y", norm_y)

    def swap_copy(half):
        return remote(
            final.at[half], other_final.at[half], swap_s.at[half], swap_r.at[half], "z", 4
        )

    SMALL = {"vy": (0, "y", conv_y), "vz": (0, "z", conv_z),
             "ny": (1, "y", norm_y), "nz": (1, "z", norm_z)}

    def small_copy(kind, half, axis, ref, shift):
        here = y if axis == "y" else z
        sem = ((kind * 2 + (axis == "z")) * 2 + half) * RING + shift
        size = 1 if kind else 8
        return remote(
            ref.at[half, RING, pl.ds(0, size), :], ref.at[half, here, pl.ds(0, size), :],
            small_s.at[sem], small_r.at[sem], axis, shift,
        )

    def small_start(kind, half, axis, ref):
        here = y if axis == "y" else z
        size = 1 if kind else 8
        for shift in FAR_FIRST:
            small_copy(kind, half, axis, ref, shift).start()
        ref[half, here, 0:size, :] = ref[half, RING, 0:size, :]

    def small_total(kind, half, ref):
        size = 1 if kind else 8
        value = ref[half, 0, 0:size, :]
        for k in range(1, RING):
            value = value + ref[half, k, 0:size, :]
        return value

    def small_on(kind, half, source, ref):
        ref[half, RING, 0 : 1 if kind else 8, :] = small_total(kind, half, source)
        small_start(kind, half, "z", ref)

    def conv_done(half):
        conv_out[:, half * HALF : (half + 1) * HALF] = small_total(0, half, conv_z)

    def norm_done(half):
        norms_out[:, half * HALF : (half + 1) * HALF] = small_total(1, half, norm_z)

    def swap_done(half):
        lanes = slice(half * HALF, (half + 1) * HALF)
        here, there = (pl.ds(pl.multiple_of(r * ROWS, ROWS), ROWS) for r in (rep, 1 - rep))
        down_out[here, lanes] = final[half]
        down_out[there, lanes] = other_final[half]

    def message(name):
        if name[0] == "g":
            return gather_copy(name[1])
        if name[0] == "c":
            return chain_copy(name[1])
        if name[0] == "x":
            return cross_copy(*name[1:])
        if name[0] == "s":
            return swap_copy(name[1])
        kind, axis, ref = SMALL[name[0]]
        return small_copy(kind, name[1], axis, ref, name[2])

    run = {
        "g": lambda k: gather_copy(k).start(),
        "f": forward, "w": weight_grad, "h": hidden_grad, "b": backward,
        "c": chain_step, "ce": chain_end, "xs": cross_start, "xe": cross_end,
        "ss": lambda half: swap_copy(half).start(), "so": swap_done,
        "ne": lambda half: small_on(1, half, norm_y, norm_z), "no": norm_done,
        "ve": lambda half: small_on(0, half, conv_y, conv_z), "vo": conv_done,
    }

    loads[0].wait()
    loads[1].wait()
    pl.semaphore_wait(barrier, 4)
    loaded = 2
    seen = []
    plan = steps()
    for name in ORDER:
        want = {"f": 8, "w": 9}.get(name[0], 0)
        for load in loads[loaded:want]:
            load.wait()
        loaded = max(loaded, want)
        for needed in plan[name][4]:
            if needed not in seen:
                message(needed).wait_recv()
                seen.append(needed)
        run[name[0]](*name[1:])
    for name in seen:
        message(name).wait_send()


def in_hbm(array):
    return pltpu.with_memory_space_constraint(array, pltpu.HBM)


def finish(gg, gl, conv, down, norms, gg_o, gl_o, tg_o, tl_o, bg_o, bl_o, down_o, norms_o, sems):
    moves = (
        (gg, gg_o), (gl, gl_o), (conv.at[pl.ds(0, 3), :], tg_o), (conv.at[pl.ds(3, 3), :], tl_o),
        (conv.at[pl.ds(6, 1), :], bg_o), (conv.at[pl.ds(7, 1), :], bl_o),
        (down, down_o), (norms, norms_o),
    )
    copies = [pltpu.make_async_copy(a, b, sems.at[k]) for k, (a, b) in enumerate(moves)]
    for copy in copies:
        copy.start()
    for copy in copies:
        copy.wait()


def local(
    pre_gate, pre_linear, taps_gate, taps_linear, bias_gate, bias_linear, down_weight, out_grad
):
    tokens, width = pre_gate.shape
    columns = out_grad.shape[1]
    any_, vmem = pl.BlockSpec(memory_space=pl.ANY), pl.BlockSpec(memory_space=pltpu.VMEM)
    hbm = pl.BlockSpec(memory_space=pltpu.HBM)
    dma = pltpu.SemaphoreType.DMA
    shape = jax.ShapeDtypeStruct
    held = pl.pallas_call(
        kernel,
        name="gated_backward",
        out_shape=(
            pltpu.VMEM((tokens, width), BF16), pltpu.VMEM((tokens, width), BF16),
            pltpu.VMEM((8, width), F32), pltpu.VMEM((BLOCK, width), F32),
            pltpu.VMEM((1, width), F32),
        ),
        in_specs=[hbm] * 8,
        out_specs=(vmem,) * 5,
        scratch_shapes=[
            pltpu.VMEM((tokens, width), BF16),
            pltpu.VMEM((tokens, width), BF16),
            pltpu.VMEM((3, width), F32),
            pltpu.VMEM((3, width), F32),
            pltpu.VMEM((1, width), F32),
            pltpu.VMEM((1, width), F32),
            pltpu.VMEM((tokens, columns), BF16),
            pltpu.VMEM((2, columns, HALF), BF16),
            pltpu.VMEM((tokens, width), BF16),
            pltpu.VMEM((tokens, width), F32),
            pltpu.VMEM((tokens, width), F32),
            pltpu.VMEM((tokens, width), F32),
            pltpu.VMEM((2, columns, HALF), F32),
            pltpu.VMEM((len(CHAIN), BLOCK, HALF), BF16),
            pltpu.VMEM((len(CHAIN), BLOCK, HALF), BF16),
            pltpu.VMEM((2, RING, ROWS, HALF), F32),
            pltpu.VMEM((2, RING, ROWS, HALF), BF16),
            pltpu.VMEM((2, RING, ROWS, HALF), BF16),
            pltpu.VMEM((2, ROWS, HALF), F32),
            pltpu.VMEM((2, ROWS, HALF), F32),
            pltpu.VMEM((width // LANES, tokens + 8, LANES), F32),
            pltpu.VMEM((width // LANES, tokens + 8, LANES), F32),
            pltpu.VMEM((width // LANES, tokens + 8, LANES), F32),
            pltpu.VMEM((width // LANES, tokens + 8, LANES), F32),
            pltpu.VMEM((8, 8, width), F32),
            pltpu.VMEM((2, RING + 1, 8, HALF), F32),
            pltpu.VMEM((2, RING + 1, 8, HALF), F32),
            pltpu.VMEM((2, RING + 1, 8, HALF), F32),
            pltpu.VMEM((2, RING + 1, 8, HALF), F32),
            dma((9,)),
            dma((len(GATHER),)), dma((len(GATHER),)),
            dma((len(CHAIN),)), dma((len(CHAIN),)),
            dma((2, RING)), dma((2, RING)),
            dma((8 * RING,)), dma((8 * RING,)),
            dma((2,)), dma((2,)),
        ],
        compiler_params=pltpu.CompilerParams(
            collective_id=0, has_side_effects=True, vmem_limit_bytes=40 * 2**20
        ),
    )(
        *map(
            in_hbm,
            (
                pre_gate, pre_linear, taps_gate, taps_linear, bias_gate.reshape(1, -1),
                bias_linear.reshape(1, -1), down_weight.T, out_grad,
            ),
        )
    )
    gg, gl, tg, tl, bg, bl, down, norms = pl.pallas_call(
        finish,
        name="finish",
        out_shape=(
            shape((tokens, width), BF16), shape((tokens, width), BF16),
            shape((3, width), F32), shape((3, width), F32),
            shape((1, width), F32), shape((1, width), F32),
            shape((BLOCK, width), F32), shape((1, width), F32),
        ),
        in_specs=[vmem] * 5,
        out_specs=(any_,) * 8,
        scratch_shapes=[dma((8,))],
        compiler_params=pltpu.CompilerParams(vmem_limit_bytes=8 * 2**20),
    )(*held)
    return gg, gl, tg, tl, bg.reshape(-1), bl.reshape(-1), down.T, norms.reshape(-1)


def solution(mesh):
    split = Mesh(
        mesh.devices.reshape(mesh.shape["rep"], 4, 8, mesh.shape["tp"]),
        ("rep", "fs_0", "fs_1", "tp"),
    )
    fs = ("fs_0", "fs_1")
    in_specs = (
        P(REP_FS, "tp"), P(REP_FS, "tp"), P(None, "tp"), P(None, "tp"),
        P("tp"), P("tp"), P("tp", fs), P(REP_FS, None),
    )
    out_specs = (
        P(REP_FS, "tp"), P(REP_FS, "tp"), P(None, "tp"), P(None, "tp"),
        P("tp"), P("tp"), P("tp", fs), P("tp"),
    )
    return jax.shard_map(local, mesh=split, in_specs=in_specs, out_specs=out_specs, check_vma=False)
```

```python
import jax
import jax.numpy as jnp
from jax import lax
from jax.experimental import pallas as pl
from jax.experimental.pallas import tpu as pltpu
from jax.sharding import Mesh
from jax.sharding import PartitionSpec as P

REP_FS = ("rep", "fs_0", "fs_1")
RING = 8
BLOCK = 64
HALF = 256
LANES = 128
ROWS = 32
F32, BF16 = jnp.float32, jnp.bfloat16
FAR_FIRST = (4, 3, 5, 2, 6, 1, 7)


def gather_messages():
    found = []

    def add(half, dz, dy, part, axis, sign, needs):
        found.append((half, dz, dy, part, axis, sign, needs))
        return len(found) - 1

    right = add(0, 0, 0, 0, "z", 1, ())
    left = add(0, 0, 0, 0, "z", -1, ())
    right2 = add(0, -1, 0, 1, "z", 1, (right,))
    left2 = add(0, 1, 0, 2, "z", -1, (left,))
    for j, (dz, needs) in enumerate(
        ((0, ()), (-1, (right,)), (1, (left,)), (2, (right2, left2)))
    ):
        for sign, hops in ((1, 4 - j % 2), (-1, 3 + j % 2)):
            before = needs
            for k in range(hops):
                before = (add(0, dz, -sign * k, 0, "y", sign, before),)
    items = [(0, ())]
    for sign, hops in ((1, 4), (-1, 3)):
        before = ()
        for k in range(hops):
            before = (add(1, 0, -sign * k, 0, "y", sign, before),)
            items.append((-sign * (k + 1), before))
    for i, (dy, needs) in enumerate(items):
        first = add(1, 0, dy, 0, "z", 1, needs)
        other = add(1, 0, dy, 0, "z", -1, needs)
        if i % 2 == 0:
            add(1, -1, dy, 0, "z", 1, (first,))
        else:
            add(1, 1, dy, 0, "z", -1, (other,))
    return found


PARTS = 4
Z_OFF = (0, 1, 3, 2)
Y_OFF = ((4, 0), (3, 5), (2, 6), (1, 7))


def chain_messages():
    return [
        (half, part, sign, step, hops)
        for half in range(2)
        for part in range(PARTS)
        for sign, hops in ((1, 4 - part % 2), (-1, 3 + part % 2))
        for step in range(hops)
    ]


GATHER = gather_messages()
CHAIN = chain_messages()
CHAIN_AT = {m[:4]: k for k, m in enumerate(CHAIN)}


def chain_ends(half, part):
    return [
        CHAIN_AT[half, part, sign, hops - 1]
        for sign, hops in ((1, 4 - part % 2), (-1, 3 + part % 2))
    ]


def cross_shifts(half, part):
    if half == 1:
        return [n for n in Y_OFF[part] if n]
    return [n for n in FAR_FIRST if n % 4 == Z_OFF[part]]


RATE, FIRST_HOP, NEXT_HOP = 44.4, 2.8, 0.8


def steps():
    found = {}

    def step(name, time, rank, after=(), needs=(), sends=(), start=0.0):
        found[name] = (time, rank, start, tuple(after), tuple(needs), tuple(sends))

    def to_all(kind, half, axis, size):
        return [
            ((kind, half, shift), axis, 1 if shift < 4 + (half == 0) else -1, size,
             min(shift, RING - shift))
            for shift in FAR_FIRST
        ]

    for i in range(4):
        step(("w", i), 0.55, 2.5, [("w", i - 1)] if i else [("f", 1, 0), ("f", 1, 1)], start=2.5)
    follow = [1] * len(GATHER)
    for k in reversed(range(len(GATHER))):
        for n in GATHER[k][6]:
            follow[n] = max(follow[n], follow[k] + 1)
    for k, (half, _, _, part, axis, sign, needs) in enumerate(GATHER):
        step(("g", k), 0.04, 0.3 - 0.01 * follow[k], (), [("g", n) for n in needs],
             [(("g", k), axis, sign, 16 if part else 32, 1)], 1.0)
    for half in range(2):
        first, second = ("y", "z") if half == 0 else ("z", "y")
        for i in range(2):
            step(("f", i, half), 0.5, 3 + i, [("f", 0, half)] * i, start=1.6 + 0.4 * i)
        for k, (h, part, sign, at, hops) in enumerate(CHAIN):
            if h == half:
                ready = ("w", part if half == 0 else Z_OFF.index(sign * (hops - at) % 4))
                step(("c", k), 0.07, 0.6 - 0.01 * (hops - at) - 0.1 * half, [ready],
                     [("c", k - 1)] * (at > 0), [(("c", k), first, sign, 128 // PARTS, 1)])
        for part in range(PARTS):
            step(("ce", half, part), 0.07, 0.2, [("w", 3)],
                 [("c", k) for k in chain_ends(half, part)])
            step(("xs", half, part), 0.02, 0.1, [("ce", half, part), ("ce", 1 - half, 0)], (),
                 [m for m in to_all("x", half, second, 16) if m[0][2] in cross_shifts(half, part)])
        step(("xe", half), 0.15, 0.1, [("xs", half, part) for part in range(PARTS)],
             [("x", half, n) for n in FAR_FIRST],
             to_all("ny", half, "y", 1))
        step(("ne", half), 0.1, 0.1, [("xe", half)], [("ny", half, n) for n in FAR_FIRST],
             to_all("nz", half, "z", 1))
        step(("no", half), 0.1, 0.1, [("ne", half)], [("nz", half, n) for n in FAR_FIRST])
        step(("ss", half), 0.02, 6, [("ne", half)], (),
             [(("s", half), "z", 1 if half else -1, 32, 4)])
        step(("so", half), 0.05, 6, [("ss", half)], [("s", half)])
        every = [("g", k) for k, m in enumerate(GATHER) if m[0] == half]
        for i in range(3):
            before = [("h", half, i - 1)] if i else every
            step(("h", half, i), 0.3, 5, before, () if i else every)
            step(("b", half, i), 0.4, 5, [("h", half, i)] + [("b", half, i - 1)] * (i > 0), (),
                 to_all("vy", half, "y", 8) if i == 2 else ())
        step(("ve", half), 0.1, 0.2, [("b", half, 2), ("ce", 1, 0)],
             [("vy", half, n) for n in FAR_FIRST], to_all("vz", half, "z", 8))
        step(("vo", half), 0.1, 0.2, [("ve", half)], [("vz", half, n) for n in FAR_FIRST])
    return found


ORDER = (
    ("g", 32), ("g", 0), ("g", 4), ("g", 8), ("g", 40), ("g", 36), ("g", 1), ("g", 39),
    ("f", 0, 0), ("f", 1, 0), ("f", 0, 1), ("f", 1, 1), ("w", 0), ("c", 4), ("c", 38), ("g", 43),
    ("c", 52), ("g", 11), ("g", 33), ("c", 0), ("g", 14), ("g", 9), ("g", 42), ("g", 2),
    ("c", 28), ("c", 42), ("w", 1), ("g", 3), ("g", 37), ("c", 32), ("c", 46), ("g", 18),
    ("c", 7), ("c", 10), ("w", 2), ("g", 41), ("c", 49), ("c", 18), ("c", 14), ("c", 35),
    ("w", 3), ("g", 55), ("c", 5), ("c", 24), ("c", 39), ("c", 21), ("g", 54), ("g", 34),
    ("g", 46), ("g", 10), ("c", 53), ("g", 45), ("c", 29), ("c", 1), ("g", 38), ("c", 43),
    ("g", 25), ("c", 33), ("c", 11), ("c", 8), ("c", 47), ("c", 19), ("c", 50), ("c", 15),
    ("g", 44), ("c", 6), ("c", 36), ("c", 22), ("c", 40), ("c", 25), ("g", 57), ("g", 35),
    ("g", 58), ("g", 28), ("g", 48), ("c", 2), ("c", 54), ("g", 22), ("c", 30), ("g", 19),
    ("c", 34), ("c", 12), ("c", 44), ("c", 9), ("c", 48), ("c", 20), ("c", 51), ("c", 16),
    ("g", 61), ("g", 15), ("c", 37), ("c", 23), ("c", 41), ("c", 26), ("g", 59), ("g", 5),
    ("g", 52), ("g", 29), ("g", 51), ("c", 3), ("c", 55), ("g", 23), ("c", 31), ("g", 20),
    ("g", 49), ("c", 13), ("c", 45), ("g", 26), ("g", 56), ("g", 60), ("c", 17), ("g", 62),
    ("g", 16), ("g", 47), ("g", 12), ("ce", 1, 1), ("c", 27), ("g", 6), ("g", 30), ("g", 53),
    ("ce", 0, 0), ("xs", 1, 1), ("ce", 1, 3), ("xs", 1, 3), ("ce", 1, 0), ("xs", 0, 0),
    ("xs", 1, 0), ("g", 50), ("ce", 0, 1), ("xs", 0, 1), ("ce", 1, 2), ("xs", 1, 2), ("ce", 0, 2),
    ("g", 27), ("xs", 0, 2), ("ce", 0, 3), ("xs", 0, 3), ("g", 13), ("g", 31), ("g", 7),
    ("h", 1, 0), ("g", 17), ("h", 1, 1), ("g", 21), ("h", 1, 2), ("g", 24), ("b", 1, 0),
    ("b", 1, 1), ("b", 1, 2), ("xe", 0), ("xe", 1), ("h", 0, 0), ("b", 0, 0), ("h", 0, 1),
    ("h", 0, 2), ("b", 0, 1), ("b", 0, 2), ("ve", 1), ("ne", 0), ("ss", 0), ("ne", 1), ("ss", 1),
    ("ve", 0), ("vo", 1), ("no", 0), ("so", 1), ("so", 0), ("no", 1), ("vo", 0),
)


def kernel(
    gate_hbm, linear_hbm, taps_g_hbm, taps_l_hbm, bias_g_hbm, bias_l_hbm, weight_hbm,
    out_grad_hbm,
    gg, gl, conv_out, down_out, norms_out,
    gate, linear, taps_g, taps_l, bias_g, bias_l, out_grad, weights, hidden, factor_g, factor_l, grad_hidden, partial,
    chain_send, chain_recv, summed, cross_send, cross_recv, final, other_final,
    rows_g, rows_l, after_g, after_l, sums, conv_y, conv_z, norm_y, norm_z,
    load_sem, gather_s, gather_r, chain_s, chain_r, cross_s, cross_r,
    small_s, small_r, swap_s, swap_r,
):
    tokens = gate_hbm.shape[0]
    rep, z_lo, y = lax.axis_index("rep"), lax.axis_index("fs_0"), lax.axis_index("fs_1")
    z = rep * 4 + z_lo

    def along(axis, shift):
        if axis == "y":
            return {"fs_1": lax.rem(y + shift + RING, RING)}
        at = lax.rem(z + shift + RING, RING)
        return {"rep": at // 4, "fs_0": lax.rem(at, 4)}

    def remote(src, dst, send, recv, axis, shift):
        return pltpu.make_async_remote_copy(
            src_ref=src, dst_ref=dst, send_sem=send, recv_sem=recv,
            device_id=along(axis, shift), device_id_type=pl.DeviceIdType.MESH,
        )

    barrier = pltpu.get_barrier_semaphore()
    for axis in ("y", "z"):
        for shift in (1, -1):
            pl.semaphore_signal(
                barrier, inc=1, device_id=along(axis, shift),
                device_id_type=pl.DeviceIdType.MESH,
            )

    own_row = pl.multiple_of((z_lo * 8 + y) * BLOCK, BLOCK)
    loads = [
        pltpu.make_async_copy(
            weight_hbm.at[:, pl.ds(h * HALF, HALF)],
            weights.at[h, pl.ds(own_row, BLOCK), :],
            load_sem.at[h],
        )
        for h in range(2)
    ]
    loads += [
        pltpu.make_async_copy(source.at[rows, :], to.at[rows, :], load_sem.at[k])
        for k, (source, to, rows) in enumerate(
            (
                (gate_hbm, gate, pl.ds(0, tokens // 2)),
                (linear_hbm, linear, pl.ds(0, tokens // 2)),
            ),
            2,
        )
    ]
    loads += [
        pltpu.make_async_copy(taps_g_hbm, taps_g, load_sem.at[5]),
        pltpu.make_async_copy(taps_l_hbm, taps_l, load_sem.at[6]),
        pltpu.make_async_copy(bias_g_hbm, bias_g, load_sem.at[7]),
        pltpu.make_async_copy(bias_l_hbm, bias_l, load_sem.at[8]),
        pltpu.make_async_copy(
            gate_hbm.at[pl.ds(tokens // 2, tokens // 2), :],
            gate.at[pl.ds(tokens // 2, tokens // 2), :],
            load_sem.at[9],
        ),
        pltpu.make_async_copy(
            linear_hbm.at[pl.ds(tokens // 2, tokens // 2), :],
            linear.at[pl.ds(tokens // 2, tokens // 2), :],
            load_sem.at[10],
        ),
        pltpu.make_async_copy(out_grad_hbm, out_grad, load_sem.at[4]),
    ]
    for load in loads:
        load.start()
    strips = rows_g.shape[0]
    for ref in (rows_g, rows_l):
        ref[:, 0:8, :] = jnp.zeros((strips, 8, LANES), F32)
    for ref in (after_g, after_l):
        ref[:, tokens : tokens + 8, :] = jnp.zeros((strips, 8, LANES), F32)

    def gather_copy(k):
        half, dz, dy, part, axis, sign, _ = GATHER[k]
        at = lax.rem(z_lo + dz + 4, 4) * 8 + lax.rem(y + dy + RING, RING)
        start, size = at * BLOCK, BLOCK
        if part:
            start, size = start + (part - 1) * 32, 32
        block = weights.at[half, pl.ds(pl.multiple_of(start, size), size), :]
        return remote(block, block, gather_s.at[k], gather_r.at[k], axis, sign)

    STEP = 64

    def strips_of(half):
        return [(n, slice(n * LANES, (n + 1) * LANES)) for n in (2 * half, 2 * half + 1)]

    def forward(seg, half):
        blocks = tokens // STEP // 2
        for n, lanes in strips_of(half):
            tg, tl = taps_g[0:3, lanes], taps_l[0:3, lanes]
            bg, bl = bias_g[0:1, lanes], bias_l[0:1, lanes]

            def convolve(source, rows, row, taps, bias):
                last = source[pl.ds(row, STEP), lanes].astype(F32)
                rows[n, pl.ds(row + 8, STEP), :] = last
                return (
                    taps[0:1] * rows[n, pl.ds(row + 6, STEP), :]
                    + taps[1:2] * rows[n, pl.ds(row + 7, STEP), :]
                    + taps[2:3] * last
                    + bias
                )

            def body(i, carry):
                row = pl.multiple_of(i * STEP, STEP)
                gate_pre = convolve(gate, rows_g, row, tg, bg)
                linear_pre = convolve(linear, rows_l, row, tl, bl)
                sigma = 1.0 / (1.0 + jnp.exp(-gate_pre))
                silu = gate_pre * sigma
                hidden[pl.ds(row, STEP), lanes] = (silu * linear_pre).astype(BF16)
                factor_g[pl.ds(row, STEP), lanes] = (
                    linear_pre * sigma * (1.0 + gate_pre * (1.0 - sigma))
                )
                factor_l[pl.ds(row, STEP), lanes] = silu
                return carry

            lax.fori_loop(seg * blocks, (seg + 1) * blocks, body, 0)

    def weight_grad(i):
        rows = pl.ds(pl.multiple_of(lax.rem(z_lo + Z_OFF[i], 4) * 512, 512), 512)
        product = lax.dot_general(
            out_grad[:, rows], hidden[...], (((0,), (0,)), ((), ())), preferred_element_type=F32
        )
        partial[0, rows, :] = product[:, :HALF]
        partial[1, rows, :] = product[:, HALF:]

    def hidden_grad(half, i):
        at, size = (2 - i) * (tokens // 3), tokens // 3
        grad_hidden[at : at + size, half * HALF : (half + 1) * HALF] = jnp.dot(
            out_grad[at : at + size, :], weights[half], preferred_element_type=F32
        )

    def fold(v):
        return jnp.sum(v.reshape(STEP // 8, 8, LANES), axis=0)

    def backward(half, seg):
        blocks = tokens // STEP // 3
        for n, lanes in strips_of(half):
            tg, tl = taps_g[0:3, lanes], taps_l[0:3, lanes]

            def back(v, after, row, taps):
                after[n, pl.ds(row, STEP), :] = v
                return (
                    taps[0:1] * after[n, pl.ds(row + 2, STEP), :]
                    + taps[1:2] * after[n, pl.ds(row + 1, STEP), :]
                    + taps[2:3] * v
                )

            def body(i, totals):
                row = pl.multiple_of((tokens // STEP - 1 - i) * STEP, STEP)
                grad = grad_hidden[pl.ds(row, STEP), lanes]
                dg = grad * factor_g[pl.ds(row, STEP), lanes]
                dl = grad * factor_l[pl.ds(row, STEP), lanes]
                gg[pl.ds(row, STEP), lanes] = back(dg, after_g, row, tg).astype(BF16)
                gl[pl.ds(row, STEP), lanes] = back(dl, after_l, row, tl).astype(BF16)
                terms = [dg * rows_g[n, pl.ds(row + 6 + j, STEP), :] for j in range(3)]
                terms += [dl * rows_l[n, pl.ds(row + 6 + j, STEP), :] for j in range(3)]
                terms += [dg, dl]
                return tuple(total + fold(term) for total, term in zip(totals, terms))

            if seg == 0:
                totals = (jnp.zeros((8, LANES), F32),) * 8
            else:
                totals = tuple(sums[j, :, lanes] for j in range(8))
            totals = lax.fori_loop(seg * blocks, (seg + 1) * blocks, body, totals)
            for j, total in enumerate(totals):
                sums[j, :, lanes] = total
        if seg == 2:
            for n, lanes in strips_of(half):
                for j in range(8):
                    total = jnp.sum(sums[j, :, lanes], axis=0, keepdims=True)
                    at = (n - 2 * half) * LANES
                    conv_y[half, RING, j : j + 1, at : at + LANES] = total
            small_start(0, half, "y", conv_y)

    def first_axis(half):
        return ("y", y) if half == 0 else ("z", z)

    def pieces(half, to, part):
        if half == 0:
            return [(lax.rem(z_lo + Z_OFF[part], 4) * 512 + to * 64, 64)]
        return [
            (lax.rem(to, 4) * 512 + lax.rem(y + n, RING) * 64 + (to // 4) * 32, 32)
            for n in Y_OFF[part]
        ]

    def chain_copy(k):
        half, part, sign, step, hops = CHAIN[k]
        return remote(
            chain_send.at[k], chain_recv.at[k], chain_s.at[k], chain_r.at[k],
            first_axis(half)[0], sign,
        )

    def chain_step(k):
        half, part, sign, step, hops = CHAIN[k]
        to = lax.rem(first_axis(half)[1] + sign * (hops - step) + RING, RING)
        at = 0
        for row, size in pieces(half, to, part):
            value = partial[half, pl.ds(pl.multiple_of(row, size), size), :]
            if step:
                value = value + chain_recv[k - 1, at : at + size, :].astype(F32)
            chain_send[k, at : at + size, :] = value.astype(BF16)
            at += size
        chain_copy(k).start()

    def chain_end(half, part):
        at = 0
        for row, size in pieces(half, first_axis(half)[1], part):
            value = partial[half, pl.ds(pl.multiple_of(row, size), size), :]
            for k in chain_ends(half, part):
                value = value + chain_recv[k, at : at + size, :].astype(F32)
            for sub in range(size // ROWS):
                slot = (part * BLOCK + at) // ROWS + sub
                piece = value[sub * ROWS : (sub + 1) * ROWS]
                summed[half, slot] = piece
                cross_send[half, slot] = piece.astype(BF16)
            at += size

    def slot_of(half, shift):
        if half == 0:
            return 2 * Z_OFF.index(shift % 4) + lax.rem(z + shift, RING) // 4
        return [n for part in Y_OFF for n in part].index(shift)

    def cross_copy(half, shift):
        slot = slot_of(half, shift)
        return remote(
            cross_send.at[half, slot], cross_recv.at[half, shift],
            cross_s.at[half, shift], cross_r.at[half, shift], "y" if half else "z", shift,
        )

    def cross_start(half, part):
        for shift in cross_shifts(half, part):
            cross_copy(half, shift).start()

    def cross_end(half):
        value = summed[half, slot_of(half, 0)]
        for shift in FAR_FIRST:
            value = value + cross_recv[half, shift].astype(F32)
        final[half] = value
        norm_y[half, RING, 0:1, :] = jnp.sum(value * value, axis=0, keepdims=True)
        small_start(1, half, "y", norm_y)

    def swap_copy(half):
        return remote(
            final.at[half], other_final.at[half], swap_s.at[half], swap_r.at[half], "z", 4
        )

    SMALL = {"vy": (0, "y", conv_y), "vz": (0, "z", conv_z),
             "ny": (1, "y", norm_y), "nz": (1, "z", norm_z)}

    def small_copy(kind, half, axis, ref, shift):
        here = y if axis == "y" else z
        sem = ((kind * 2 + (axis == "z")) * 2 + half) * RING + shift
        size = 1 if kind else 8
        return remote(
            ref.at[half, RING, pl.ds(0, size), :], ref.at[half, here, pl.ds(0, size), :],
            small_s.at[sem], small_r.at[sem], axis, shift,
        )

    def small_start(kind, half, axis, ref):
        here = y if axis == "y" else z
        size = 1 if kind else 8
        for shift in FAR_FIRST:
            small_copy(kind, half, axis, ref, shift).start()
        ref[half, here, 0:size, :] = ref[half, RING, 0:size, :]

    def small_total(kind, half, ref):
        size = 1 if kind else 8
        value = ref[half, 0, 0:size, :]
        for k in range(1, RING):
            value = value + ref[half, k, 0:size, :]
        return value

    def small_on(kind, half, source, ref):
        ref[half, RING, 0 : 1 if kind else 8, :] = small_total(kind, half, source)
        small_start(kind, half, "z", ref)

    def conv_done(half):
        conv_out[:, half * HALF : (half + 1) * HALF] = small_total(0, half, conv_z)

    def norm_done(half):
        norms_out[:, half * HALF : (half + 1) * HALF] = small_total(1, half, norm_z)

    def swap_done(half):
        lanes = slice(half * HALF, (half + 1) * HALF)
        here, there = (pl.ds(pl.multiple_of(r * ROWS, ROWS), ROWS) for r in (rep, 1 - rep))
        down_out[here, lanes] = final[half]
        down_out[there, lanes] = other_final[half]

    def message(name):
        if name[0] == "g":
            return gather_copy(name[1])
        if name[0] == "c":
            return chain_copy(name[1])
        if name[0] == "x":
            return cross_copy(*name[1:])
        if name[0] == "s":
            return swap_copy(name[1])
        kind, axis, ref = SMALL[name[0]]
        return small_copy(kind, name[1], axis, ref, name[2])

    run = {
        "g": lambda k: gather_copy(k).start(),
        "f": forward, "w": weight_grad, "h": hidden_grad, "b": backward,
        "c": chain_step, "ce": chain_end, "xs": cross_start, "xe": cross_end,
        "ss": lambda half: swap_copy(half).start(), "so": swap_done,
        "ne": lambda half: small_on(1, half, norm_y, norm_z), "no": norm_done,
        "ve": lambda half: small_on(0, half, conv_y, conv_z), "vo": conv_done,
    }

    loads[0].wait()
    loads[1].wait()
    pl.semaphore_wait(barrier, 4)
    loaded = 2
    seen = []
    plan = steps()
    for name in ORDER:
        want = {"f": 8 + 2 * name[1], "w": 11}.get(name[0], 0)
        for load in loads[loaded:want]:
            load.wait()
        loaded = max(loaded, want)
        for needed in plan[name][4]:
            if needed not in seen:
                message(needed).wait_recv()
                seen.append(needed)
        run[name[0]](*name[1:])
    for name in seen:
        message(name).wait_send()


def in_hbm(array):
    return pltpu.with_memory_space_constraint(array, pltpu.HBM)


def finish(gg, gl, conv, down, norms, gg_o, gl_o, tg_o, tl_o, bg_o, bl_o, down_o, norms_o, sems):
    moves = (
        (gg, gg_o), (gl, gl_o), (conv.at[pl.ds(0, 3), :], tg_o), (conv.at[pl.ds(3, 3), :], tl_o),
        (conv.at[pl.ds(6, 1), :], bg_o), (conv.at[pl.ds(7, 1), :], bl_o),
        (down, down_o), (norms, norms_o),
    )
    copies = [pltpu.make_async_copy(a, b, sems.at[k]) for k, (a, b) in enumerate(moves)]
    for copy in copies:
        copy.start()
    for copy in copies:
        copy.wait()


def local(
    pre_gate, pre_linear, taps_gate, taps_linear, bias_gate, bias_linear, down_weight, out_grad
):
    tokens, width = pre_gate.shape
    columns = out_grad.shape[1]
    any_, vmem = pl.BlockSpec(memory_space=pl.ANY), pl.BlockSpec(memory_space=pltpu.VMEM)
    hbm = pl.BlockSpec(memory_space=pltpu.HBM)
    dma = pltpu.SemaphoreType.DMA
    shape = jax.ShapeDtypeStruct
    held = pl.pallas_call(
        kernel,
        name="gated_backward",
        out_shape=(
            pltpu.VMEM((tokens, width), BF16), pltpu.VMEM((tokens, width), BF16),
            pltpu.VMEM((8, width), F32), pltpu.VMEM((BLOCK, width), F32),
            pltpu.VMEM((1, width), F32),
        ),
        in_specs=[hbm] * 8,
        out_specs=(vmem,) * 5,
        scratch_shapes=[
            pltpu.VMEM((tokens, width), BF16),
            pltpu.VMEM((tokens, width), BF16),
            pltpu.VMEM((3, width), F32),
            pltpu.VMEM((3, width), F32),
            pltpu.VMEM((1, width), F32),
            pltpu.VMEM((1, width), F32),
            pltpu.VMEM((tokens, columns), BF16),
            pltpu.VMEM((2, columns, HALF), BF16),
            pltpu.VMEM((tokens, width), BF16),
            pltpu.VMEM((tokens, width), F32),
            pltpu.VMEM((tokens, width), F32),
            pltpu.VMEM((tokens, width), F32),
            pltpu.VMEM((2, columns, HALF), F32),
            pltpu.VMEM((len(CHAIN), BLOCK, HALF), BF16),
            pltpu.VMEM((len(CHAIN), BLOCK, HALF), BF16),
            pltpu.VMEM((2, RING, ROWS, HALF), F32),
            pltpu.VMEM((2, RING, ROWS, HALF), BF16),
            pltpu.VMEM((2, RING, ROWS, HALF), BF16),
            pltpu.VMEM((2, ROWS, HALF), F32),
            pltpu.VMEM((2, ROWS, HALF), F32),
            pltpu.VMEM((width // LANES, tokens + 8, LANES), F32),
            pltpu.VMEM((width // LANES, tokens + 8, LANES), F32),
            pltpu.VMEM((width // LANES, tokens + 8, LANES), F32),
            pltpu.VMEM((width // LANES, tokens + 8, LANES), F32),
            pltpu.VMEM((8, 8, width), F32),
            pltpu.VMEM((2, RING + 1, 8, HALF), F32),
            pltpu.VMEM((2, RING + 1, 8, HALF), F32),
            pltpu.VMEM((2, RING + 1, 8, HALF), F32),
            pltpu.VMEM((2, RING + 1, 8, HALF), F32),
            dma((11,)),
            dma((len(GATHER),)), dma((len(GATHER),)),
            dma((len(CHAIN),)), dma((len(CHAIN),)),
            dma((2, RING)), dma((2, RING)),
            dma((8 * RING,)), dma((8 * RING,)),
            dma((2,)), dma((2,)),
        ],
        compiler_params=pltpu.CompilerParams(
            collective_id=0, has_side_effects=True, vmem_limit_bytes=40 * 2**20
        ),
    )(
        *map(
            in_hbm,
            (
                pre_gate, pre_linear, taps_gate, taps_linear, bias_gate.reshape(1, -1),
                bias_linear.reshape(1, -1), down_weight.T, out_grad,
            ),
        )
    )
    gg, gl, tg, tl, bg, bl, down, norms = pl.pallas_call(
        finish,
        name="finish",
        out_shape=(
            shape((tokens, width), BF16), shape((tokens, width), BF16),
            shape((3, width), F32), shape((3, width), F32),
            shape((1, width), F32), shape((1, width), F32),
            shape((BLOCK, width), F32), shape((1, width), F32),
        ),
        in_specs=[vmem] * 5,
        out_specs=(any_,) * 8,
        scratch_shapes=[dma((8,))],
        compiler_params=pltpu.CompilerParams(vmem_limit_bytes=8 * 2**20),
    )(*held)
    return gg, gl, tg, tl, bg.reshape(-1), bl.reshape(-1), down.T, norms.reshape(-1)


def solution(mesh):
    split = Mesh(
        mesh.devices.reshape(mesh.shape["rep"], 4, 8, mesh.shape["tp"]),
        ("rep", "fs_0", "fs_1", "tp"),
    )
    fs = ("fs_0", "fs_1")
    in_specs = (
        P(REP_FS, "tp"), P(REP_FS, "tp"), P(None, "tp"), P(None, "tp"),
        P("tp"), P("tp"), P("tp", fs), P(REP_FS, None),
    )
    out_specs = (
        P(REP_FS, "tp"), P(REP_FS, "tp"), P(None, "tp"), P(None, "tp"),
        P("tp"), P("tp"), P("tp", fs), P("tp"),
    )
    return jax.shard_map(local, mesh=split, in_specs=in_specs, out_specs=out_specs, check_vma=False)
```

```python
import jax
import jax.numpy as jnp
from jax import lax
from jax.experimental import pallas as pl
from jax.experimental.pallas import tpu as pltpu
from jax.sharding import Mesh
from jax.sharding import PartitionSpec as P

REP_FS = ("rep", "fs_0", "fs_1")
RING = 8
BLOCK = 64
HALF = 256
LANES = 128
ROWS = 32
F32, BF16 = jnp.float32, jnp.bfloat16
FAR_FIRST = (4, 3, 5, 2, 6, 1, 7)


def gather_messages():
    found = []

    def add(half, dz, dy, part, axis, sign, needs):
        found.append((half, dz, dy, part, axis, sign, needs))
        return len(found) - 1

    right = add(0, 0, 0, 0, "z", 1, ())
    left = add(0, 0, 0, 0, "z", -1, ())
    right2 = add(0, -1, 0, 1, "z", 1, (right,))
    left2 = add(0, 1, 0, 2, "z", -1, (left,))
    for j, (dz, needs) in enumerate(
        ((0, ()), (-1, (right,)), (1, (left,)), (2, (right2, left2)))
    ):
        for sign, hops in ((1, 4 - j % 2), (-1, 3 + j % 2)):
            before = needs
            for k in range(hops):
                before = (add(0, dz, -sign * k, 0, "y", sign, before),)
    items = [(0, ())]
    for sign, hops in ((1, 4), (-1, 3)):
        before = ()
        for k in range(hops):
            before = (add(1, 0, -sign * k, 0, "y", sign, before),)
            items.append((-sign * (k + 1), before))
    for i, (dy, needs) in enumerate(items):
        first = add(1, 0, dy, 0, "z", 1, needs)
        other = add(1, 0, dy, 0, "z", -1, needs)
        if i % 2 == 0:
            add(1, -1, dy, 0, "z", 1, (first,))
        else:
            add(1, 1, dy, 0, "z", -1, (other,))
    return found


PARTS = 4
Z_OFF = (0, 1, 3, 2)
Y_OFF = ((4, 0), (3, 5), (2, 6), (1, 7))


def chain_messages():
    return [
        (half, part, sign, step, hops)
        for half in range(2)
        for part in range(PARTS)
        for sign, hops in ((1, 4 - part % 2), (-1, 3 + part % 2))
        for step in range(hops)
    ]


GATHER = gather_messages()
CHAIN = chain_messages()
CHAIN_AT = {m[:4]: k for k, m in enumerate(CHAIN)}


def chain_ends(half, part):
    return [
        CHAIN_AT[half, part, sign, hops - 1]
        for sign, hops in ((1, 4 - part % 2), (-1, 3 + part % 2))
    ]


def cross_shifts(half, part):
    if half == 1:
        return [n for n in Y_OFF[part] if n]
    return [n for n in FAR_FIRST if n % 4 == Z_OFF[part]]


RATE, FIRST_HOP, NEXT_HOP = 44.4, 2.8, 0.8


def steps():
    found = {}

    def step(name, time, rank, after=(), needs=(), sends=(), start=0.0):
        found[name] = (time, rank, start, tuple(after), tuple(needs), tuple(sends))

    def to_all(kind, half, axis, size):
        return [
            ((kind, half, shift), axis, 1 if shift < 4 + (half == 0) else -1, size,
             min(shift, RING - shift))
            for shift in FAR_FIRST
        ]

    for i in range(4):
        step(("w", i), 0.5, 2.5, [("w", i - 1)] if i else [("f", 1, 0), ("f", 1, 1)], start=2.5)
    follow = [1] * len(GATHER)
    for k in reversed(range(len(GATHER))):
        for n in GATHER[k][6]:
            follow[n] = max(follow[n], follow[k] + 1)
    for k, (half, _, _, part, axis, sign, needs) in enumerate(GATHER):
        step(("g", k), 0.04, 0.3 - 0.01 * follow[k], (), [("g", n) for n in needs],
             [(("g", k), axis, sign, 16 if part else 32, 1)], 1.0)
    for half in range(2):
        first, second = ("y", "z") if half == 0 else ("z", "y")
        for i in range(2):
            step(("f", i, half), 0.44, 3 + i, [("f", 0, half)] * i, start=1.6 + 0.4 * i)
        for k, (h, part, sign, at, hops) in enumerate(CHAIN):
            if h == half:
                ready = ("w", part if half == 0 else Z_OFF.index(sign * (hops - at) % 4))
                step(("c", k), 0.07, 0.6 - 0.01 * (hops - at) - 0.1 * half, [ready],
                     [("c", k - 1)] * (at > 0), [(("c", k), first, sign, 128 // PARTS, 1)])
        for part in range(PARTS):
            step(("ce", half, part), 0.07, 0.2, [("w", 3)],
                 [("c", k) for k in chain_ends(half, part)])
            step(("xs", half, part), 0.02, 0.1, [("ce", half, part), ("ce", 1 - half, 0)], (),
                 [m for m in to_all("x", half, second, 16) if m[0][2] in cross_shifts(half, part)])
        step(("xe", half), 0.15, 0.1, [("xs", half, part) for part in range(PARTS)],
             [("x", half, n) for n in FAR_FIRST],
             to_all("ny", half, "y", 1))
        step(("ne", half), 0.1, 0.1, [("xe", half)], [("ny", half, n) for n in FAR_FIRST],
             to_all("nz", half, "z", 1))
        step(("no", half), 0.1, 0.1, [("ne", half)], [("nz", half, n) for n in FAR_FIRST])
        step(("ss", half), 0.02, 6, [("ne", half)], (),
             [(("s", half), "z", 1 if half else -1, 32, 4)])
        step(("so", half), 0.05, 6, [("ss", half)], [("s", half)])
        every = [("g", k) for k, m in enumerate(GATHER) if m[0] == half]
        for i in range(3):
            before = [("h", half, i - 1)] if i else every
            step(("h", half, i), 0.3, 5, before, () if i else every)
            step(("b", half, i), 0.35, 5, [("h", half, i)] + [("b", half, i - 1)] * (i > 0), (),
                 to_all("vy", half, "y", 8) if i == 2 else ())
        step(("ve", half), 0.1, 0.2, [("b", half, 2), ("ce", 1, 0)],
             [("vy", half, n) for n in FAR_FIRST], to_all("vz", half, "z", 8))
        step(("vo", half), 0.1, 0.2, [("ve", half)], [("vz", half, n) for n in FAR_FIRST])
    return found


ORDER = (
    ("g", 40), ("g", 36), ("g", 0), ("g", 1), ("g", 8), ("g", 32), ("g", 39), ("g", 4),
    ("f", 0, 1), ("f", 0, 0), ("f", 1, 0), ("f", 1, 1), ("w", 0), ("c", 0), ("c", 4), ("c", 38),
    ("c", 28), ("g", 37), ("g", 11), ("g", 55), ("g", 2), ("g", 33), ("c", 52), ("g", 54),
    ("c", 42), ("g", 14), ("w", 1), ("g", 5), ("c", 7), ("g", 3), ("c", 46), ("g", 22), ("c", 32),
    ("c", 10), ("w", 2), ("c", 14), ("c", 35), ("c", 18), ("c", 49), ("w", 3), ("c", 24),
    ("c", 21), ("g", 43), ("c", 1), ("c", 5), ("g", 42), ("c", 39), ("c", 29), ("g", 56),
    ("g", 45), ("c", 53), ("g", 34), ("g", 38), ("c", 43), ("g", 18), ("g", 28), ("c", 47),
    ("c", 36), ("c", 8), ("c", 11), ("c", 33), ("c", 50), ("c", 15), ("c", 19), ("g", 46),
    ("c", 22), ("g", 57), ("c", 25), ("c", 40), ("c", 30), ("c", 2), ("c", 6), ("g", 58),
    ("g", 48), ("g", 35), ("g", 15), ("c", 54), ("c", 44), ("g", 25), ("g", 29), ("c", 48),
    ("c", 37), ("c", 9), ("c", 12), ("c", 34), ("c", 51), ("c", 16), ("c", 20), ("g", 49),
    ("c", 23), ("g", 60), ("c", 26), ("c", 41), ("c", 31), ("c", 3), ("g", 23), ("g", 61),
    ("g", 51), ("g", 19), ("g", 16), ("c", 55), ("c", 45), ("g", 26), ("g", 30), ("g", 52),
    ("g", 47), ("c", 13), ("g", 12), ("g", 44), ("c", 17), ("g", 41), ("g", 9), ("g", 50),
    ("g", 59), ("c", 27), ("g", 6), ("ce", 1, 1), ("ce", 1, 0), ("ce", 0, 0), ("xs", 0, 0),
    ("xs", 1, 0), ("xs", 1, 1), ("g", 62), ("ce", 1, 3), ("g", 20), ("xs", 1, 3), ("ce", 1, 2),
    ("xs", 1, 2), ("g", 53), ("ce", 0, 1), ("xs", 0, 1), ("ce", 0, 2), ("xs", 0, 2), ("g", 13),
    ("ce", 0, 3), ("xs", 0, 3), ("g", 27), ("g", 17), ("g", 7), ("g", 10), ("g", 31), ("g", 21),
    ("h", 1, 0), ("h", 1, 1), ("g", 24), ("b", 1, 0), ("b", 1, 1), ("h", 1, 2), ("b", 1, 2),
    ("xe", 1), ("xe", 0), ("h", 0, 0), ("h", 0, 1), ("h", 0, 2), ("b", 0, 0), ("b", 0, 1),
    ("b", 0, 2), ("ve", 1), ("ne", 0), ("ss", 0), ("ne", 1), ("ss", 1), ("ve", 0), ("vo", 1),
    ("no", 0), ("so", 1), ("so", 0), ("no", 1), ("vo", 0),
)


def kernel(
    gate_hbm, linear_hbm, taps_g_hbm, taps_l_hbm, bias_g_hbm, bias_l_hbm, weight_hbm,
    out_grad_hbm,
    gg, gl, conv_out, down_out, norms_out,
    gate, linear, taps_g, taps_l, bias_g, bias_l, out_grad, weights, hidden, factor_g, factor_l, grad_hidden, partial,
    chain_send, chain_recv, summed, cross_send, cross_recv, final, other_final,
    rows_g, rows_l, after_g, after_l, sums, conv_y, conv_z, norm_y, norm_z,
    load_sem, gather_s, gather_r, chain_s, chain_r, cross_s, cross_r,
    small_s, small_r, swap_s, swap_r,
):
    tokens = gate_hbm.shape[0]
    rep, z_lo, y = lax.axis_index("rep"), lax.axis_index("fs_0"), lax.axis_index("fs_1")
    z = rep * 4 + z_lo

    def along(axis, shift):
        if axis == "y":
            return {"fs_1": lax.rem(y + shift + RING, RING)}
        at = lax.rem(z + shift + RING, RING)
        return {"rep": at // 4, "fs_0": lax.rem(at, 4)}

    def remote(src, dst, send, recv, axis, shift):
        return pltpu.make_async_remote_copy(
            src_ref=src, dst_ref=dst, send_sem=send, recv_sem=recv,
            device_id=along(axis, shift), device_id_type=pl.DeviceIdType.MESH,
        )

    barrier = pltpu.get_barrier_semaphore()
    for axis in ("y", "z"):
        for shift in (1, -1):
            pl.semaphore_signal(
                barrier, inc=1, device_id=along(axis, shift),
                device_id_type=pl.DeviceIdType.MESH,
            )

    own_row = pl.multiple_of((z_lo * 8 + y) * BLOCK, BLOCK)
    loads = [
        pltpu.make_async_copy(
            weight_hbm.at[:, pl.ds(h * HALF, HALF)],
            weights.at[h, pl.ds(own_row, BLOCK), :],
            load_sem.at[h],
        )
        for h in range(2)
    ]
    loads += [
        pltpu.make_async_copy(source.at[rows, :], to.at[rows, :], load_sem.at[k])
        for k, (source, to, rows) in enumerate(
            (
                (gate_hbm, gate, pl.ds(0, tokens // 2)),
                (linear_hbm, linear, pl.ds(0, tokens // 2)),
            ),
            2,
        )
    ]
    loads += [
        pltpu.make_async_copy(taps_g_hbm, taps_g, load_sem.at[5]),
        pltpu.make_async_copy(taps_l_hbm, taps_l, load_sem.at[6]),
        pltpu.make_async_copy(bias_g_hbm, bias_g, load_sem.at[7]),
        pltpu.make_async_copy(bias_l_hbm, bias_l, load_sem.at[8]),
        pltpu.make_async_copy(
            gate_hbm.at[pl.ds(tokens // 2, tokens // 2), :],
            gate.at[pl.ds(tokens // 2, tokens // 2), :],
            load_sem.at[9],
        ),
        pltpu.make_async_copy(
            linear_hbm.at[pl.ds(tokens // 2, tokens // 2), :],
            linear.at[pl.ds(tokens // 2, tokens // 2), :],
            load_sem.at[10],
        ),
        pltpu.make_async_copy(out_grad_hbm, out_grad, load_sem.at[4]),
    ]
    for load in loads:
        load.start()
    strips = rows_g.shape[0]
    for ref in (rows_g, rows_l):
        ref[:, 0:8, :] = jnp.zeros((strips, 8, LANES), F32)
    for ref in (after_g, after_l):
        ref[:, tokens : tokens + 8, :] = jnp.zeros((strips, 8, LANES), F32)

    def gather_copy(k):
        half, dz, dy, part, axis, sign, _ = GATHER[k]
        at = lax.rem(z_lo + dz + 4, 4) * 8 + lax.rem(y + dy + RING, RING)
        start, size = at * BLOCK, BLOCK
        if part:
            start, size = start + (part - 1) * 32, 32
        block = weights.at[half, pl.ds(pl.multiple_of(start, size), size), :]
        return remote(block, block, gather_s.at[k], gather_r.at[k], axis, sign)

    STEP = 64

    def strips_of(half):
        return [(n, slice(n * LANES, (n + 1) * LANES)) for n in (2 * half, 2 * half + 1)]

    def forward(seg, half):
        blocks = tokens // STEP // 2
        for n, lanes in strips_of(half):
            tg, tl = taps_g[0:3, lanes], taps_l[0:3, lanes]
            bg, bl = bias_g[0:1, lanes], bias_l[0:1, lanes]

            def convolve(source, rows, row, taps, bias):
                last = source[pl.ds(row, STEP), lanes].astype(F32)
                rows[n, pl.ds(row + 8, STEP), :] = last
                return (
                    taps[0:1] * rows[n, pl.ds(row + 6, STEP), :]
                    + taps[1:2] * rows[n, pl.ds(row + 7, STEP), :]
                    + taps[2:3] * last
                    + bias
                )

            def body(i, carry):
                row = pl.multiple_of(i * STEP, STEP)
                gate_pre = convolve(gate, rows_g, row, tg, bg)
                linear_pre = convolve(linear, rows_l, row, tl, bl)
                sigma = 1.0 / (1.0 + jnp.exp(-gate_pre))
                silu = gate_pre * sigma
                hidden[pl.ds(row, STEP), lanes] = (silu * linear_pre).astype(BF16)
                factor_g[pl.ds(row, STEP), lanes] = (
                    linear_pre * sigma * (1.0 + gate_pre * (1.0 - sigma))
                )
                factor_l[pl.ds(row, STEP), lanes] = silu
                return carry

            lax.fori_loop(seg * blocks, (seg + 1) * blocks, body, 0)

    def weight_grad(i):
        rows = pl.ds(pl.multiple_of(lax.rem(z_lo + Z_OFF[i], 4) * 512, 512), 512)
        product = lax.dot_general(
            out_grad[:, rows], hidden[...], (((0,), (0,)), ((), ())), preferred_element_type=F32
        )
        partial[0, rows, :] = product[:, :HALF]
        partial[1, rows, :] = product[:, HALF:]

    def hidden_grad(half, i):
        at, size = (2 - i) * (tokens // 3), tokens // 3
        grad_hidden[at : at + size, half * HALF : (half + 1) * HALF] = jnp.dot(
            out_grad[at : at + size, :], weights[half], preferred_element_type=F32
        )

    def fold(v):
        return jnp.sum(v.reshape(STEP // 8, 8, LANES), axis=0)

    def backward(half, seg):
        blocks = tokens // STEP // 3
        for n, lanes in strips_of(half):
            tg, tl = taps_g[0:3, lanes], taps_l[0:3, lanes]

            def back(v, after, row, taps):
                after[n, pl.ds(row, STEP), :] = v
                return (
                    taps[0:1] * after[n, pl.ds(row + 2, STEP), :]
                    + taps[1:2] * after[n, pl.ds(row + 1, STEP), :]
                    + taps[2:3] * v
                )

            def body(i, totals):
                row = pl.multiple_of((tokens // STEP - 1 - i) * STEP, STEP)
                grad = grad_hidden[pl.ds(row, STEP), lanes]
                dg = grad * factor_g[pl.ds(row, STEP), lanes]
                dl = grad * factor_l[pl.ds(row, STEP), lanes]
                gg[pl.ds(row, STEP), lanes] = back(dg, after_g, row, tg).astype(BF16)
                gl[pl.ds(row, STEP), lanes] = back(dl, after_l, row, tl).astype(BF16)
                terms = [dg * rows_g[n, pl.ds(row + 6 + j, STEP), :] for j in range(3)]
                terms += [dl * rows_l[n, pl.ds(row + 6 + j, STEP), :] for j in range(3)]
                terms += [dg, dl]
                return tuple(total + fold(term) for total, term in zip(totals, terms))

            if seg == 0:
                totals = (jnp.zeros((8, LANES), F32),) * 8
            else:
                totals = tuple(sums[j, :, lanes] for j in range(8))
            totals = lax.fori_loop(seg * blocks, (seg + 1) * blocks, body, totals)
            for j, total in enumerate(totals):
                sums[j, :, lanes] = total
        if seg == 2:
            for n, lanes in strips_of(half):
                for j in range(8):
                    total = jnp.sum(sums[j, :, lanes], axis=0, keepdims=True)
                    at = (n - 2 * half) * LANES
                    conv_y[half, RING, j : j + 1, at : at + LANES] = total
            small_start(0, half, "y", conv_y)

    def first_axis(half):
        return ("y", y) if half == 0 else ("z", z)

    def pieces(half, to, part):
        if half == 0:
            return [(lax.rem(z_lo + Z_OFF[part], 4) * 512 + to * 64, 64)]
        return [
            (lax.rem(to, 4) * 512 + lax.rem(y + n, RING) * 64 + (to // 4) * 32, 32)
            for n in Y_OFF[part]
        ]

    def chain_copy(k):
        half, part, sign, step, hops = CHAIN[k]
        return remote(
            chain_send.at[k], chain_recv.at[k], chain_s.at[k], chain_r.at[k],
            first_axis(half)[0], sign,
        )

    def chain_step(k):
        half, part, sign, step, hops = CHAIN[k]
        to = lax.rem(first_axis(half)[1] + sign * (hops - step) + RING, RING)
        at = 0
        for row, size in pieces(half, to, part):
            value = partial[half, pl.ds(pl.multiple_of(row, size), size), :]
            if step:
                value = value + chain_recv[k - 1, at : at + size, :].astype(F32)
            chain_send[k, at : at + size, :] = value.astype(BF16)
            at += size
        chain_copy(k).start()

    def chain_end(half, part):
        at = 0
        for row, size in pieces(half, first_axis(half)[1], part):
            value = partial[half, pl.ds(pl.multiple_of(row, size), size), :]
            for k in chain_ends(half, part):
                value = value + chain_recv[k, at : at + size, :].astype(F32)
            for sub in range(size // ROWS):
                slot = (part * BLOCK + at) // ROWS + sub
                piece = value[sub * ROWS : (sub + 1) * ROWS]
                summed[half, slot] = piece
                cross_send[half, slot] = piece.astype(BF16)
            at += size

    def slot_of(half, shift):
        if half == 0:
            return 2 * Z_OFF.index(shift % 4) + lax.rem(z + shift, RING) // 4
        return [n for part in Y_OFF for n in part].index(shift)

    def cross_copy(half, shift):
        slot = slot_of(half, shift)
        return remote(
            cross_send.at[half, slot], cross_recv.at[half, shift],
            cross_s.at[half, shift], cross_r.at[half, shift], "y" if half else "z", shift,
        )

    def cross_start(half, part):
        for shift in cross_shifts(half, part):
            cross_copy(half, shift).start()

    def cross_end(half):
        value = summed[half, slot_of(half, 0)]
        for shift in FAR_FIRST:
            value = value + cross_recv[half, shift].astype(F32)
        final[half] = value
        norm_y[half, RING, 0:1, :] = jnp.sum(value * value, axis=0, keepdims=True)
        small_start(1, half, "y", norm_y)

    def swap_copy(half):
        return remote(
            final.at[half], other_final.at[half], swap_s.at[half], swap_r.at[half], "z", 4
        )

    SMALL = {"vy": (0, "y", conv_y), "vz": (0, "z", conv_z),
             "ny": (1, "y", norm_y), "nz": (1, "z", norm_z)}

    def small_copy(kind, half, axis, ref, shift):
        here = y if axis == "y" else z
        sem = ((kind * 2 + (axis == "z")) * 2 + half) * RING + shift
        size = 1 if kind else 8
        return remote(
            ref.at[half, RING, pl.ds(0, size), :], ref.at[half, here, pl.ds(0, size), :],
            small_s.at[sem], small_r.at[sem], axis, shift,
        )

    def small_start(kind, half, axis, ref):
        here = y if axis == "y" else z
        size = 1 if kind else 8
        for shift in FAR_FIRST:
            small_copy(kind, half, axis, ref, shift).start()
        ref[half, here, 0:size, :] = ref[half, RING, 0:size, :]

    def small_total(kind, half, ref):
        size = 1 if kind else 8
        value = ref[half, 0, 0:size, :]
        for k in range(1, RING):
            value = value + ref[half, k, 0:size, :]
        return value

    def small_on(kind, half, source, ref):
        ref[half, RING, 0 : 1 if kind else 8, :] = small_total(kind, half, source)
        small_start(kind, half, "z", ref)

    def conv_done(half):
        conv_out[:, half * HALF : (half + 1) * HALF] = small_total(0, half, conv_z)

    def norm_done(half):
        norms_out[:, half * HALF : (half + 1) * HALF] = small_total(1, half, norm_z)

    def swap_done(half):
        lanes = slice(half * HALF, (half + 1) * HALF)
        here, there = (pl.ds(pl.multiple_of(r * ROWS, ROWS), ROWS) for r in (rep, 1 - rep))
        down_out[here, lanes] = final[half]
        down_out[there, lanes] = other_final[half]

    def message(name):
        if name[0] == "g":
            return gather_copy(name[1])
        if name[0] == "c":
            return chain_copy(name[1])
        if name[0] == "x":
            return cross_copy(*name[1:])
        if name[0] == "s":
            return swap_copy(name[1])
        kind, axis, ref = SMALL[name[0]]
        return small_copy(kind, name[1], axis, ref, name[2])

    run = {
        "g": lambda k: gather_copy(k).start(),
        "f": forward, "w": weight_grad, "h": hidden_grad, "b": backward,
        "c": chain_step, "ce": chain_end, "xs": cross_start, "xe": cross_end,
        "ss": lambda half: swap_copy(half).start(), "so": swap_done,
        "ne": lambda half: small_on(1, half, norm_y, norm_z), "no": norm_done,
        "ve": lambda half: small_on(0, half, conv_y, conv_z), "vo": conv_done,
    }

    loads[0].wait()
    loads[1].wait()
    pl.semaphore_wait(barrier, 4)
    loaded = 2
    seen = []
    plan = steps()
    for name in ORDER:
        want = {"f": 8 + 2 * name[1], "w": 11}.get(name[0], 0)
        for load in loads[loaded:want]:
            load.wait()
        loaded = max(loaded, want)
        for needed in plan[name][4]:
            if needed not in seen:
                message(needed).wait_recv()
                seen.append(needed)
        run[name[0]](*name[1:])
    for name in seen:
        message(name).wait_send()


def in_hbm(array):
    return pltpu.with_memory_space_constraint(array, pltpu.HBM)


def finish(gg, gl, conv, down, norms, gg_o, gl_o, tg_o, tl_o, bg_o, bl_o, down_o, norms_o, sems):
    moves = (
        (gg, gg_o), (gl, gl_o), (conv.at[pl.ds(0, 3), :], tg_o), (conv.at[pl.ds(3, 3), :], tl_o),
        (conv.at[pl.ds(6, 1), :], bg_o), (conv.at[pl.ds(7, 1), :], bl_o),
        (down, down_o), (norms, norms_o),
    )
    copies = [pltpu.make_async_copy(a, b, sems.at[k]) for k, (a, b) in enumerate(moves)]
    for copy in copies:
        copy.start()
    for copy in copies:
        copy.wait()


def local(
    pre_gate, pre_linear, taps_gate, taps_linear, bias_gate, bias_linear, down_weight, out_grad
):
    tokens, width = pre_gate.shape
    columns = out_grad.shape[1]
    any_, vmem = pl.BlockSpec(memory_space=pl.ANY), pl.BlockSpec(memory_space=pltpu.VMEM)
    hbm = pl.BlockSpec(memory_space=pltpu.HBM)
    dma = pltpu.SemaphoreType.DMA
    shape = jax.ShapeDtypeStruct
    held = pl.pallas_call(
        kernel,
        name="gated_backward",
        out_shape=(
            pltpu.VMEM((tokens, width), BF16), pltpu.VMEM((tokens, width), BF16),
            pltpu.VMEM((8, width), F32), pltpu.VMEM((BLOCK, width), F32),
            pltpu.VMEM((1, width), F32),
        ),
        in_specs=[hbm] * 8,
        out_specs=(vmem,) * 5,
        scratch_shapes=[
            pltpu.VMEM((tokens, width), BF16),
            pltpu.VMEM((tokens, width), BF16),
            pltpu.VMEM((3, width), F32),
            pltpu.VMEM((3, width), F32),
            pltpu.VMEM((1, width), F32),
            pltpu.VMEM((1, width), F32),
            pltpu.VMEM((tokens, columns), BF16),
            pltpu.VMEM((2, columns, HALF), BF16),
            pltpu.VMEM((tokens, width), BF16),
            pltpu.VMEM((tokens, width), F32),
            pltpu.VMEM((tokens, width), F32),
            pltpu.VMEM((tokens, width), F32),
            pltpu.VMEM((2, columns, HALF), F32),
            pltpu.VMEM((len(CHAIN), BLOCK, HALF), BF16),
            pltpu.VMEM((len(CHAIN), BLOCK, HALF), BF16),
            pltpu.VMEM((2, RING, ROWS, HALF), F32),
            pltpu.VMEM((2, RING, ROWS, HALF), BF16),
            pltpu.VMEM((2, RING, ROWS, HALF), BF16),
            pltpu.VMEM((2, ROWS, HALF), F32),
            pltpu.VMEM((2, ROWS, HALF), F32),
            pltpu.VMEM((width // LANES, tokens + 8, LANES), F32),
            pltpu.VMEM((width // LANES, tokens + 8, LANES), F32),
            pltpu.VMEM((width // LANES, tokens + 8, LANES), F32),
            pltpu.VMEM((width // LANES, tokens + 8, LANES), F32),
            pltpu.VMEM((8, 8, width), F32),
            pltpu.VMEM((2, RING + 1, 8, HALF), F32),
            pltpu.VMEM((2, RING + 1, 8, HALF), F32),
            pltpu.VMEM((2, RING + 1, 8, HALF), F32),
            pltpu.VMEM((2, RING + 1, 8, HALF), F32),
            dma((11,)),
            dma((len(GATHER),)), dma((len(GATHER),)),
            dma((len(CHAIN),)), dma((len(CHAIN),)),
            dma((2, RING)), dma((2, RING)),
            dma((8 * RING,)), dma((8 * RING,)),
            dma((2,)), dma((2,)),
        ],
        compiler_params=pltpu.CompilerParams(
            collective_id=0, has_side_effects=True, vmem_limit_bytes=40 * 2**20
        ),
    )(
        *map(
            in_hbm,
            (
                pre_gate, pre_linear, taps_gate, taps_linear, bias_gate.reshape(1, -1),
                bias_linear.reshape(1, -1), down_weight.T, out_grad,
            ),
        )
    )
    gg, gl, tg, tl, bg, bl, down, norms = pl.pallas_call(
        finish,
        name="finish",
        out_shape=(
            shape((tokens, width), BF16), shape((tokens, width), BF16),
            shape((3, width), F32), shape((3, width), F32),
            shape((1, width), F32), shape((1, width), F32),
            shape((BLOCK, width), F32), shape((1, width), F32),
        ),
        in_specs=[vmem] * 5,
        out_specs=(any_,) * 8,
        scratch_shapes=[dma((8,))],
        compiler_params=pltpu.CompilerParams(vmem_limit_bytes=8 * 2**20),
    )(*held)
    return gg, gl, tg, tl, bg.reshape(-1), bl.reshape(-1), down.T, norms.reshape(-1)


def solution(mesh):
    split = Mesh(
        mesh.devices.reshape(mesh.shape["rep"], 4, 8, mesh.shape["tp"]),
        ("rep", "fs_0", "fs_1", "tp"),
    )
    fs = ("fs_0", "fs_1")
    in_specs = (
        P(REP_FS, "tp"), P(REP_FS, "tp"), P(None, "tp"), P(None, "tp"),
        P("tp"), P("tp"), P("tp", fs), P(REP_FS, None),
    )
    out_specs = (
        P(REP_FS, "tp"), P(REP_FS, "tp"), P(None, "tp"), P(None, "tp"),
        P("tp"), P("tp"), P("tp", fs), P("tp"),
    )
    return jax.shard_map(local, mesh=split, in_specs=in_specs, out_specs=out_specs, check_vma=False)
```

```python
import jax
import jax.numpy as jnp
from jax import lax
from jax.experimental import pallas as pl
from jax.experimental.pallas import tpu as pltpu
from jax.sharding import Mesh
from jax.sharding import PartitionSpec as P

REP_FS = ("rep", "fs_0", "fs_1")
RING = 8
BLOCK = 64
HALF = 256
LANES = 128
ROWS = 32
F32, BF16 = jnp.float32, jnp.bfloat16
FAR_FIRST = (4, 3, 5, 2, 6, 1, 7)


def gather_messages():
    found = []

    def add(half, dz, dy, part, axis, sign, needs):
        found.append((half, dz, dy, part, axis, sign, needs))
        return len(found) - 1

    right = add(0, 0, 0, 0, "z", 1, ())
    left = add(0, 0, 0, 0, "z", -1, ())
    right2 = add(0, -1, 0, 1, "z", 1, (right,))
    left2 = add(0, 1, 0, 2, "z", -1, (left,))
    for j, (dz, needs) in enumerate(
        ((0, ()), (-1, (right,)), (1, (left,)), (2, (right2, left2)))
    ):
        for sign, hops in ((1, 4 - j % 2), (-1, 3 + j % 2)):
            before = needs
            for k in range(hops):
                before = (add(0, dz, -sign * k, 0, "y", sign, before),)
    items = [(0, ())]
    for sign, hops in ((1, 4), (-1, 3)):
        before = ()
        for k in range(hops):
            before = (add(1, 0, -sign * k, 0, "y", sign, before),)
            items.append((-sign * (k + 1), before))
    for i, (dy, needs) in enumerate(items):
        first = add(1, 0, dy, 0, "z", 1, needs)
        other = add(1, 0, dy, 0, "z", -1, needs)
        if i % 2 == 0:
            add(1, -1, dy, 0, "z", 1, (first,))
        else:
            add(1, 1, dy, 0, "z", -1, (other,))
    return found


PARTS = 4
Z_OFF = (0, 1, 3, 2)
Y_OFF = ((4, 0), (3, 5), (2, 6), (1, 7))


def chain_messages():
    return [
        (half, part, sign, step, hops)
        for half in range(2)
        for part in range(PARTS)
        for sign, hops in ((1, 4 - part % 2), (-1, 3 + part % 2))
        for step in range(hops)
    ]


GATHER = gather_messages()
CHAIN = chain_messages()
CHAIN_AT = {m[:4]: k for k, m in enumerate(CHAIN)}


def chain_ends(half, part):
    return [
        CHAIN_AT[half, part, sign, hops - 1]
        for sign, hops in ((1, 4 - part % 2), (-1, 3 + part % 2))
    ]


def cross_shifts(half, part):
    if half == 1:
        return [n for n in Y_OFF[part] if n]
    return [n for n in FAR_FIRST if n % 4 == Z_OFF[part]]


RATE, FIRST_HOP, NEXT_HOP = 44.4, 2.8, 0.8


def steps():
    found = {}

    def step(name, time, rank, after=(), needs=(), sends=(), start=0.0):
        found[name] = (time, rank, start, tuple(after), tuple(needs), tuple(sends))

    def to_all(kind, half, axis, size):
        return [
            ((kind, half, shift), axis, 1 if shift < 4 + (half == 0) else -1, size,
             min(shift, RING - shift))
            for shift in FAR_FIRST
        ]

    for i in range(4):
        step(("w", i), 0.5, 2.5, [("w", i - 1)] if i else [("f", 1, 0), ("f", 1, 1)], start=2.5)
    follow = [1] * len(GATHER)
    for k in reversed(range(len(GATHER))):
        for n in GATHER[k][6]:
            follow[n] = max(follow[n], follow[k] + 1)
    for k, (half, _, _, part, axis, sign, needs) in enumerate(GATHER):
        step(("g", k), 0.04, 0.3 - 0.01 * follow[k], (), [("g", n) for n in needs],
             [(("g", k), axis, sign, 16 if part else 32, 1)], 1.0)
    for half in range(2):
        first, second = ("y", "z") if half == 0 else ("z", "y")
        for i in range(2):
            step(("f", i, half), 0.44, 3 + i, [("f", 0, half)] * i, start=1.6 + 0.4 * i)
        for k, (h, part, sign, at, hops) in enumerate(CHAIN):
            if h == half:
                ready = ("w", part if half == 0 else Z_OFF.index(sign * (hops - at) % 4))
                step(("c", k), 0.07, 0.6 - 0.01 * (hops - at) - 0.1 * half, [ready],
                     [("c", k - 1)] * (at > 0), [(("c", k), first, sign, 128 // PARTS, 1)])
        for part in range(PARTS):
            step(("ce", half, part), 0.07, 0.2, [("w", 3)],
                 [("c", k) for k in chain_ends(half, part)])
            step(("xs", half, part), 0.02, 0.1, [("ce", half, part), ("ce", 1 - half, 0)], (),
                 [m for m in to_all("x", half, second, 16) if m[0][2] in cross_shifts(half, part)])
        step(("xe", half), 0.15, 0.1, [("xs", half, part) for part in range(PARTS)],
             [("x", half, n) for n in FAR_FIRST],
             to_all("ny", half, "y", 1))
        step(("ne", half), 0.1, 0.1, [("xe", half)], [("ny", half, n) for n in FAR_FIRST],
             to_all("nz", half, "z", 1))
        step(("no", half), 0.1, 0.1, [("ne", half)], [("nz", half, n) for n in FAR_FIRST])
        step(("ss", half), 0.02, 6, [("ne", half)], (),
             [(("s", half), "z", 1 if half else -1, 32, 4)])
        step(("so", half), 0.05, 6, [("ss", half)], [("s", half)])
        every = [("g", k) for k, m in enumerate(GATHER) if m[0] == half]
        for i in range(3):
            before = [("h", half, i - 1)] if i else every
            step(("h", half, i), 0.3, 5, before, () if i else every)
            step(("b", half, i), 0.35, 5, [("h", half, i)] + [("b", half, i - 1)] * (i > 0), (),
                 to_all("vy", half, "y", 8) if i == 2 else ())
        step(("ve", half), 0.1, 0.2, [("b", half, 2), ("ce", 1, 0)],
             [("vy", half, n) for n in FAR_FIRST], to_all("vz", half, "z", 8))
        step(("vo", half), 0.1, 0.2, [("ve", half)], [("vz", half, n) for n in FAR_FIRST])
    return found


ORDER = (
    ("g", 40), ("g", 36), ("g", 0), ("g", 1), ("g", 8), ("g", 32), ("g", 39), ("g", 4),
    ("f", 0, 1), ("f", 0, 0), ("f", 1, 0), ("f", 1, 1), ("w", 0), ("c", 0), ("c", 4), ("c", 38),
    ("c", 28), ("g", 37), ("g", 11), ("g", 55), ("g", 2), ("g", 33), ("c", 52), ("g", 54),
    ("c", 42), ("g", 14), ("w", 1), ("g", 5), ("c", 7), ("g", 3), ("c", 46), ("g", 22), ("c", 32),
    ("c", 10), ("w", 2), ("c", 14), ("c", 35), ("c", 18), ("c", 49), ("w", 3), ("c", 24),
    ("c", 21), ("g", 43), ("c", 1), ("c", 5), ("g", 42), ("c", 39), ("c", 29), ("g", 56),
    ("g", 45), ("c", 53), ("g", 34), ("g", 38), ("c", 43), ("g", 18), ("g", 28), ("c", 47),
    ("c", 36), ("c", 8), ("c", 11), ("c", 33), ("c", 50), ("c", 15), ("c", 19), ("g", 46),
    ("c", 22), ("g", 57), ("c", 25), ("c", 40), ("c", 30), ("c", 2), ("c", 6), ("g", 58),
    ("g", 48), ("g", 35), ("g", 15), ("c", 54), ("c", 44), ("g", 25), ("g", 29), ("c", 48),
    ("c", 37), ("c", 9), ("c", 12), ("c", 34), ("c", 51), ("c", 16), ("c", 20), ("g", 49),
    ("c", 23), ("g", 60), ("c", 26), ("c", 41), ("c", 31), ("c", 3), ("g", 23), ("g", 61),
    ("g", 51), ("g", 19), ("g", 16), ("c", 55), ("c", 45), ("g", 26), ("g", 30), ("g", 52),
    ("g", 47), ("c", 13), ("g", 12), ("g", 44), ("c", 17), ("g", 41), ("g", 9), ("g", 50),
    ("g", 59), ("c", 27), ("g", 6), ("ce", 1, 1), ("ce", 1, 0), ("ce", 0, 0), ("xs", 0, 0),
    ("xs", 1, 0), ("xs", 1, 1), ("g", 62), ("ce", 1, 3), ("g", 20), ("xs", 1, 3), ("ce", 1, 2),
    ("xs", 1, 2), ("g", 53), ("ce", 0, 1), ("xs", 0, 1), ("ce", 0, 2), ("xs", 0, 2), ("g", 13),
    ("ce", 0, 3), ("xs", 0, 3), ("g", 27), ("g", 17), ("g", 7), ("g", 10), ("g", 31), ("g", 21),
    ("h", 1, 0), ("h", 1, 1), ("g", 24), ("b", 1, 0), ("b", 1, 1), ("h", 1, 2), ("b", 1, 2),
    ("xe", 1), ("xe", 0), ("h", 0, 0), ("h", 0, 1), ("h", 0, 2), ("b", 0, 0), ("b", 0, 1),
    ("b", 0, 2), ("ve", 1), ("ne", 0), ("ss", 0), ("ne", 1), ("ss", 1), ("ve", 0), ("vo", 1),
    ("no", 0), ("so", 1), ("so", 0), ("no", 1), ("vo", 0),
)


def kernel(
    gate_hbm, linear_hbm, taps_g_hbm, taps_l_hbm, bias_g_hbm, bias_l_hbm, weight_hbm,
    out_grad_hbm,
    gg, gl, conv_out, down_out, norms_out,
    gate, linear, taps_g, taps_l, bias_g, bias_l, out_grad, weights, hidden, factor_g, factor_l, grad_hidden, partial,
    chain_send, chain_recv, summed, cross_send, cross_recv, final, other_final,
    rows_g, rows_l, after_g, after_l, sums, conv_y, conv_z, norm_y, norm_z,
    load_sem, gather_s, gather_r, chain_s, chain_r, cross_s, cross_r,
    small_s, small_r, swap_s, swap_r,
):
    tokens = gate_hbm.shape[0]
    rep, z_lo, y = lax.axis_index("rep"), lax.axis_index("fs_0"), lax.axis_index("fs_1")
    z = rep * 4 + z_lo

    def along(axis, shift):
        if axis == "y":
            return {"fs_1": lax.rem(y + shift + RING, RING)}
        at = lax.rem(z + shift + RING, RING)
        return {"rep": at // 4, "fs_0": lax.rem(at, 4)}

    def remote(src, dst, send, recv, axis, shift):
        return pltpu.make_async_remote_copy(
            src_ref=src, dst_ref=dst, send_sem=send, recv_sem=recv,
            device_id=along(axis, shift), device_id_type=pl.DeviceIdType.MESH,
        )

    barrier = pltpu.get_barrier_semaphore()
    for axis in ("y", "z"):
        for shift in (1, -1):
            pl.semaphore_signal(
                barrier, inc=1, device_id=along(axis, shift),
                device_id_type=pl.DeviceIdType.MESH,
            )

    own_row = pl.multiple_of((z_lo * 8 + y) * BLOCK, BLOCK)
    loads = [
        pltpu.make_async_copy(
            weight_hbm.at[:, pl.ds(h * HALF, HALF)],
            weights.at[h, pl.ds(own_row, BLOCK), :],
            load_sem.at[h],
        )
        for h in range(2)
    ]
    loads += [
        pltpu.make_async_copy(source.at[rows, :], to.at[rows, :], load_sem.at[k])
        for k, (source, to, rows) in enumerate(
            (
                (gate_hbm, gate, pl.ds(0, tokens // 2)),
                (linear_hbm, linear, pl.ds(0, tokens // 2)),
            ),
            2,
        )
    ]
    loads += [
        pltpu.make_async_copy(taps_g_hbm, taps_g, load_sem.at[5]),
        pltpu.make_async_copy(taps_l_hbm, taps_l, load_sem.at[6]),
        pltpu.make_async_copy(bias_g_hbm, bias_g, load_sem.at[7]),
        pltpu.make_async_copy(bias_l_hbm, bias_l, load_sem.at[8]),
        pltpu.make_async_copy(
            gate_hbm.at[pl.ds(tokens // 2, tokens // 2), :],
            gate.at[pl.ds(tokens // 2, tokens // 2), :],
            load_sem.at[9],
        ),
        pltpu.make_async_copy(
            linear_hbm.at[pl.ds(tokens // 2, tokens // 2), :],
            linear.at[pl.ds(tokens // 2, tokens // 2), :],
            load_sem.at[10],
        ),
        pltpu.make_async_copy(out_grad_hbm, out_grad, load_sem.at[4]),
    ]
    for load in loads:
        load.start()
    strips = rows_g.shape[0]
    for ref in (rows_g, rows_l):
        ref[:, 0:8, :] = jnp.zeros((strips, 8, LANES), F32)
    for ref in (after_g, after_l):
        ref[:, tokens : tokens + 8, :] = jnp.zeros((strips, 8, LANES), F32)

    def gather_copy(k):
        half, dz, dy, part, axis, sign, _ = GATHER[k]
        at = lax.rem(z_lo + dz + 4, 4) * 8 + lax.rem(y + dy + RING, RING)
        start, size = at * BLOCK, BLOCK
        if part:
            start, size = start + (part - 1) * 32, 32
        block = weights.at[half, pl.ds(pl.multiple_of(start, size), size), :]
        return remote(block, block, gather_s.at[k], gather_r.at[k], axis, sign)

    STEP = 64

    def strips_of(half):
        return [(n, slice(n * LANES, (n + 1) * LANES)) for n in (2 * half, 2 * half + 1)]

    def forward(seg, half):
        blocks = tokens // STEP // 2
        for n, lanes in strips_of(half):
            tg, tl = taps_g[0:3, lanes], taps_l[0:3, lanes]
            bg, bl = bias_g[0:1, lanes], bias_l[0:1, lanes]

            def convolve(source, rows, row, taps, bias):
                last = source[pl.ds(row, STEP), lanes].astype(F32)
                rows[n, pl.ds(row + 8, STEP), :] = last
                return (
                    taps[0:1] * rows[n, pl.ds(row + 6, STEP), :]
                    + taps[1:2] * rows[n, pl.ds(row + 7, STEP), :]
                    + taps[2:3] * last
                    + bias
                )

            def body(i, carry):
                row = pl.multiple_of(i * STEP, STEP)
                gate_pre = convolve(gate, rows_g, row, tg, bg)
                linear_pre = convolve(linear, rows_l, row, tl, bl)
                sigma = 1.0 / (1.0 + jnp.exp(-gate_pre))
                silu = gate_pre * sigma
                hidden[pl.ds(row, STEP), lanes] = (silu * linear_pre).astype(BF16)
                factor_g[pl.ds(row, STEP), lanes] = (
                    linear_pre * sigma * (1.0 + gate_pre * (1.0 - sigma))
                )
                factor_l[pl.ds(row, STEP), lanes] = silu
                return carry

            lax.fori_loop(seg * blocks, (seg + 1) * blocks, body, 0)

    def weight_grad(i):
        rows = pl.ds(pl.multiple_of(lax.rem(z_lo + Z_OFF[i], 4) * 512, 512), 512)
        product = lax.dot_general(
            out_grad[:, rows], hidden[...], (((0,), (0,)), ((), ())), preferred_element_type=F32
        )
        partial[0, rows, :] = product[:, :HALF]
        partial[1, rows, :] = product[:, HALF:]

    def hidden_grad(half, i):
        at, size = (2 - i) * (tokens // 3), tokens // 3
        grad_hidden[at : at + size, half * HALF : (half + 1) * HALF] = jnp.dot(
            out_grad[at : at + size, :], weights[half], preferred_element_type=F32
        )

    def fold(v):
        return jnp.sum(v.reshape(STEP // 8, 8, LANES), axis=0)

    def backward(half, seg):
        blocks = tokens // STEP // 3
        for n, lanes in strips_of(half):
            tg, tl = taps_g[0:3, lanes], taps_l[0:3, lanes]

            def back(v, after, row, taps):
                after[n, pl.ds(row, STEP), :] = v
                return (
                    taps[0:1] * after[n, pl.ds(row + 2, STEP), :]
                    + taps[1:2] * after[n, pl.ds(row + 1, STEP), :]
                    + taps[2:3] * v
                )

            def body(i, totals):
                row = pl.multiple_of((tokens // STEP - 1 - i) * STEP, STEP)
                grad = grad_hidden[pl.ds(row, STEP), lanes]
                dg = grad * factor_g[pl.ds(row, STEP), lanes]
                dl = grad * factor_l[pl.ds(row, STEP), lanes]
                gg[pl.ds(row, STEP), lanes] = back(dg, after_g, row, tg).astype(BF16)
                gl[pl.ds(row, STEP), lanes] = back(dl, after_l, row, tl).astype(BF16)
                terms = [dg * rows_g[n, pl.ds(row + 6 + j, STEP), :] for j in range(3)]
                terms += [dl * rows_l[n, pl.ds(row + 6 + j, STEP), :] for j in range(3)]
                terms += [dg, dl]
                return tuple(total + fold(term) for total, term in zip(totals, terms))

            if seg == 0:
                totals = (jnp.zeros((8, LANES), F32),) * 8
            else:
                totals = tuple(sums[j, :, lanes] for j in range(8))
            totals = lax.fori_loop(seg * blocks, (seg + 1) * blocks, body, totals)
            for j, total in enumerate(totals):
                sums[j, :, lanes] = total
        if seg == 2:
            for n, lanes in strips_of(half):
                for j in range(8):
                    total = jnp.sum(sums[j, :, lanes], axis=0, keepdims=True)
                    at = (n - 2 * half) * LANES
                    conv_y[half, RING, j : j + 1, at : at + LANES] = total
            small_start(0, half, "y", conv_y)

    def first_axis(half):
        return ("y", y) if half == 0 else ("z", z)

    def pieces(half, to, part):
        if half == 0:
            return [(lax.rem(z_lo + Z_OFF[part], 4) * 512 + to * 64, 64)]
        return [
            (lax.rem(to, 4) * 512 + lax.rem(y + n, RING) * 64 + (to // 4) * 32, 32)
            for n in Y_OFF[part]
        ]

    def chain_copy(k):
        half, part, sign, step, hops = CHAIN[k]
        return remote(
            chain_send.at[k], chain_recv.at[k], chain_s.at[k], chain_r.at[k],
            first_axis(half)[0], sign,
        )

    def chain_step(k):
        half, part, sign, step, hops = CHAIN[k]
        to = lax.rem(first_axis(half)[1] + sign * (hops - step) + RING, RING)
        at = 0
        for row, size in pieces(half, to, part):
            value = partial[half, pl.ds(pl.multiple_of(row, size), size), :]
            if step:
                value = value + chain_recv[k - 1, at : at + size, :].astype(F32)
            chain_send[k, at : at + size, :] = value.astype(BF16)
            at += size
        chain_copy(k).start()

    def chain_end(half, part):
        at = 0
        for row, size in pieces(half, first_axis(half)[1], part):
            value = partial[half, pl.ds(pl.multiple_of(row, size), size), :]
            for k in chain_ends(half, part):
                value = value + chain_recv[k, at : at + size, :].astype(F32)
            for sub in range(size // ROWS):
                slot = (part * BLOCK + at) // ROWS + sub
                piece = value[sub * ROWS : (sub + 1) * ROWS]
                summed[half, slot] = piece
                cross_send[half, slot] = piece.astype(BF16)
            at += size

    def slot_of(half, shift):
        if half == 0:
            return 2 * Z_OFF.index(shift % 4) + lax.rem(z + shift, RING) // 4
        return [n for part in Y_OFF for n in part].index(shift)

    def cross_copy(half, shift):
        slot = slot_of(half, shift)
        return remote(
            cross_send.at[half, slot], cross_recv.at[half, shift],
            cross_s.at[half, shift], cross_r.at[half, shift], "y" if half else "z", shift,
        )

    def cross_start(half, part):
        for shift in cross_shifts(half, part):
            cross_copy(half, shift).start()

    def cross_end(half):
        value = summed[half, slot_of(half, 0)]
        for shift in FAR_FIRST:
            value = value + cross_recv[half, shift].astype(F32)
        final[half] = value
        norm_y[half, RING, 0:1, :] = jnp.sum(value * value, axis=0, keepdims=True)
        small_start(1, half, "y", norm_y)

    def swap_copy(half):
        return remote(
            final.at[half], other_final.at[half], swap_s.at[half], swap_r.at[half], "z", 4
        )

    SMALL = {"vy": (0, "y", conv_y), "vz": (0, "z", conv_z),
             "ny": (1, "y", norm_y), "nz": (1, "z", norm_z)}

    def small_copy(kind, half, axis, ref, shift):
        here = y if axis == "y" else z
        sem = ((kind * 2 + (axis == "z")) * 2 + half) * RING + shift
        size = 1 if kind else 8
        return remote(
            ref.at[half, RING, pl.ds(0, size), :], ref.at[half, here, pl.ds(0, size), :],
            small_s.at[sem], small_r.at[sem], axis, shift,
        )

    def small_start(kind, half, axis, ref):
        here = y if axis == "y" else z
        size = 1 if kind else 8
        for shift in FAR_FIRST:
            small_copy(kind, half, axis, ref, shift).start()
        ref[half, here, 0:size, :] = ref[half, RING, 0:size, :]

    def small_total(kind, half, ref):
        size = 1 if kind else 8
        value = ref[half, 0, 0:size, :]
        for k in range(1, RING):
            value = value + ref[half, k, 0:size, :]
        return value

    def small_on(kind, half, source, ref):
        ref[half, RING, 0 : 1 if kind else 8, :] = small_total(kind, half, source)
        small_start(kind, half, "z", ref)

    def conv_done(half):
        conv_out[:, half * HALF : (half + 1) * HALF] = small_total(0, half, conv_z)

    def norm_done(half):
        norms_out[:, half * HALF : (half + 1) * HALF] = small_total(1, half, norm_z)

    def swap_done(half):
        lanes = slice(half * HALF, (half + 1) * HALF)
        here, there = (pl.ds(pl.multiple_of(r * ROWS, ROWS), ROWS) for r in (rep, 1 - rep))
        down_out[here, lanes] = final[half]
        down_out[there, lanes] = other_final[half]

    def message(name):
        if name[0] == "g":
            return gather_copy(name[1])
        if name[0] == "c":
            return chain_copy(name[1])
        if name[0] == "x":
            return cross_copy(*name[1:])
        if name[0] == "s":
            return swap_copy(name[1])
        kind, axis, ref = SMALL[name[0]]
        return small_copy(kind, name[1], axis, ref, name[2])

    run = {
        "g": lambda k: gather_copy(k).start(),
        "f": forward, "w": weight_grad, "h": hidden_grad, "b": backward,
        "c": chain_step, "ce": chain_end, "xs": cross_start, "xe": cross_end,
        "ss": lambda half: swap_copy(half).start(), "so": swap_done,
        "ne": lambda half: small_on(1, half, norm_y, norm_z), "no": norm_done,
        "ve": lambda half: small_on(0, half, conv_y, conv_z), "vo": conv_done,
    }

    loads[0].wait()
    loads[1].wait()
    pl.semaphore_wait(barrier, 4)
    loaded = 2
    seen, sent = [], []
    plan = steps()
    for name in ORDER:
        if name[0] in ("no", "vo", "so"):
            for done in [n for n in seen if n not in sent]:
                message(done).wait_send()
                sent.append(done)
        want = {"f": 8 + 2 * name[1], "w": 11}.get(name[0], 0)
        for load in loads[loaded:want]:
            load.wait()
        loaded = max(loaded, want)
        for needed in plan[name][4]:
            if needed not in seen:
                message(needed).wait_recv()
                seen.append(needed)
        run[name[0]](*name[1:])
    for name in [n for n in seen if n not in sent]:
        message(name).wait_send()


def in_hbm(array):
    return pltpu.with_memory_space_constraint(array, pltpu.HBM)


def finish(gg, gl, conv, down, norms, gg_o, gl_o, tg_o, tl_o, bg_o, bl_o, down_o, norms_o, sems):
    moves = (
        (gg, gg_o), (gl, gl_o), (conv.at[pl.ds(0, 3), :], tg_o), (conv.at[pl.ds(3, 3), :], tl_o),
        (conv.at[pl.ds(6, 1), :], bg_o), (conv.at[pl.ds(7, 1), :], bl_o),
        (down, down_o), (norms, norms_o),
    )
    copies = [pltpu.make_async_copy(a, b, sems.at[k]) for k, (a, b) in enumerate(moves)]
    for copy in copies:
        copy.start()
    for copy in copies:
        copy.wait()


def local(
    pre_gate, pre_linear, taps_gate, taps_linear, bias_gate, bias_linear, down_weight, out_grad
):
    tokens, width = pre_gate.shape
    columns = out_grad.shape[1]
    any_, vmem = pl.BlockSpec(memory_space=pl.ANY), pl.BlockSpec(memory_space=pltpu.VMEM)
    hbm = pl.BlockSpec(memory_space=pltpu.HBM)
    dma = pltpu.SemaphoreType.DMA
    shape = jax.ShapeDtypeStruct
    held = pl.pallas_call(
        kernel,
        name="gated_backward",
        out_shape=(
            pltpu.VMEM((tokens, width), BF16), pltpu.VMEM((tokens, width), BF16),
            pltpu.VMEM((8, width), F32), pltpu.VMEM((BLOCK, width), F32),
            pltpu.VMEM((1, width), F32),
        ),
        in_specs=[hbm] * 8,
        out_specs=(vmem,) * 5,
        scratch_shapes=[
            pltpu.VMEM((tokens, width), BF16),
            pltpu.VMEM((tokens, width), BF16),
            pltpu.VMEM((3, width), F32),
            pltpu.VMEM((3, width), F32),
            pltpu.VMEM((1, width), F32),
            pltpu.VMEM((1, width), F32),
            pltpu.VMEM((tokens, columns), BF16),
            pltpu.VMEM((2, columns, HALF), BF16),
            pltpu.VMEM((tokens, width), BF16),
            pltpu.VMEM((tokens, width), F32),
            pltpu.VMEM((tokens, width), F32),
            pltpu.VMEM((tokens, width), F32),
            pltpu.VMEM((2, columns, HALF), F32),
            pltpu.VMEM((len(CHAIN), BLOCK, HALF), BF16),
            pltpu.VMEM((len(CHAIN), BLOCK, HALF), BF16),
            pltpu.VMEM((2, RING, ROWS, HALF), F32),
            pltpu.VMEM((2, RING, ROWS, HALF), BF16),
            pltpu.VMEM((2, RING, ROWS, HALF), BF16),
            pltpu.VMEM((2, ROWS, HALF), F32),
            pltpu.VMEM((2, ROWS, HALF), F32),
            pltpu.VMEM((width // LANES, tokens + 8, LANES), F32),
            pltpu.VMEM((width // LANES, tokens + 8, LANES), F32),
            pltpu.VMEM((width // LANES, tokens + 8, LANES), F32),
            pltpu.VMEM((width // LANES, tokens + 8, LANES), F32),
            pltpu.VMEM((8, 8, width), F32),
            pltpu.VMEM((2, RING + 1, 8, HALF), F32),
            pltpu.VMEM((2, RING + 1, 8, HALF), F32),
            pltpu.VMEM((2, RING + 1, 8, HALF), F32),
            pltpu.VMEM((2, RING + 1, 8, HALF), F32),
            dma((11,)),
            dma((len(GATHER),)), dma((len(GATHER),)),
            dma((len(CHAIN),)), dma((len(CHAIN),)),
            dma((2, RING)), dma((2, RING)),
            dma((8 * RING,)), dma((8 * RING,)),
            dma((2,)), dma((2,)),
        ],
        compiler_params=pltpu.CompilerParams(
            collective_id=0, has_side_effects=True, vmem_limit_bytes=40 * 2**20
        ),
    )(
        *map(
            in_hbm,
            (
                pre_gate, pre_linear, taps_gate, taps_linear, bias_gate.reshape(1, -1),
                bias_linear.reshape(1, -1), down_weight.T, out_grad,
            ),
        )
    )
    gg, gl, tg, tl, bg, bl, down, norms = pl.pallas_call(
        finish,
        name="finish",
        out_shape=(
            shape((tokens, width), BF16), shape((tokens, width), BF16),
            shape((3, width), F32), shape((3, width), F32),
            shape((1, width), F32), shape((1, width), F32),
            shape((BLOCK, width), F32), shape((1, width), F32),
        ),
        in_specs=[vmem] * 5,
        out_specs=(any_,) * 8,
        scratch_shapes=[dma((8,))],
        compiler_params=pltpu.CompilerParams(vmem_limit_bytes=8 * 2**20),
    )(*held)
    return gg, gl, tg, tl, bg.reshape(-1), bl.reshape(-1), down.T, norms.reshape(-1)


def solution(mesh):
    split = Mesh(
        mesh.devices.reshape(mesh.shape["rep"], 4, 8, mesh.shape["tp"]),
        ("rep", "fs_0", "fs_1", "tp"),
    )
    fs = ("fs_0", "fs_1")
    in_specs = (
        P(REP_FS, "tp"), P(REP_FS, "tp"), P(None, "tp"), P(None, "tp"),
        P("tp"), P("tp"), P("tp", fs), P(REP_FS, None),
    )
    out_specs = (
        P(REP_FS, "tp"), P(REP_FS, "tp"), P(None, "tp"), P(None, "tp"),
        P("tp"), P("tp"), P("tp", fs), P("tp"),
    )
    return jax.shard_map(local, mesh=split, in_specs=in_specs, out_specs=out_specs, check_vma=False)
```
